32 devices in a mesh: sp: 4 (over z), fs: 4 (over y, x), tp: 2 (over core).
Axes of the slice: x: 2, y: 2, z: 4, core: 2. Of those that a mesh axis runs over, the one named last changes fastest.
Arguments:
- state_head_inputs: bfloat16 [4, 512, 1024], P('fs', 'sp', 'tp'), may hold values from -6 to 6
- state_write_vectors: bfloat16 [4, 512, 256], P('fs', 'sp', 'tp'), may hold values from -3 to 3
- state_read_vectors: bfloat16 [4, 512, 256], P('fs', 'sp', 'tp'), may hold values from -3 to 3
- state_output_gate: bfloat16 [4, 512, 1024], P('fs', 'sp', 'tp'), may hold values from -6 to 6
- presoftplus_steps: float32 [4, 16, 512], P('fs', 'tp', 'sp'), may hold values from -6 to 6
- extra_decay_log: float32 [4, 16, 512], P('fs', 'tp', 'sp'), may hold values from -2.1 to 0, as said below
- lane_shrinkage_powers: float32 [16], P('tp')
- bypass_coefficient_vector: float32 [16], P('tp'), may hold values from 0.5 to 4
- feeder_smoothing_stencil: bfloat16 [4, 1024], P(None, 'tp'), may hold values from -3 to 3
- stored_smoothing_stencil: bfloat16 [4, 256], P(None, 'tp'), may hold values from -3 to 3
- lookup_smoothing_stencil: bfloat16 [4, 256], P(None, 'tp'), may hold values from -3 to 3
- bundled_rescaling_vector: float32 [1024], P('tp'), may hold values from 0.1 to 1.9
- queries: bfloat16 [4, 512, 1024], P('fs', 'sp', 'tp'), may hold values from -8 to 8
- attention_keys: bfloat16 [4, 512, 256], P('fs', 'sp', 'tp'), may hold values from -8 to 8
- attention_values: bfloat16 [4, 512, 256], P('fs', 'sp', 'tp'), may hold values from -6 to 6
- forget_gate_cumsum: float32 [4, 512, 16], P('fs', 'sp', 'tp'), as said below
- state_out_weight: bfloat16 [1024, 2048], P('tp', 'fs'), may hold values from -0.1875 to 0.1875
- attention_out_weight: bfloat16 [1024, 2048], P('tp', 'fs'), may hold values from -0.75 to 0.75
Outputs:
- layer_output: bfloat16 [4, 512, 2048], P('fs', ('sp', 'tp'))
The draws below stay inside these ranges and needn't reach their ends.
Inputs may be any that keep to these rules, and one draw needn't show every extreme that they name: `extra_decay_log`: nonpositive. `forget_gate_cumsum`: never rises along the positions of a sequence.
All inputs are finite; a program needn't handle non-finite values.
Results may differ from the reference program's by a relative error of at most 0.019.
Values may be sent and summed in bfloat16 or wider, within the bound.
A program may use at most 64 MiB of HBM per device.

```python
import math
import jax
import jax.numpy as jnp
from jax import lax

D = 2048
SPACE_MODEL_LANES = 16
FOX_QUESTIONERS = 16
KV_HEADS = 4
HEAD_DIM = 64
STATE = 128
GROUPS = 2
CONV = 4
TOKENS_PER_SHARD = 128
SEQS = 4
LENGTH = 512
SSD_WIDTH = 1024
FOX_WIDTH = 1024


def fast_rate():
    return 1.0 / min(40, max(TOKENS_PER_SHARD // 4, 2))


def head_rates(plain_quantity, lane_tally):
    order_key, slow_key, quick_key = jax.random.split(plain_quantity, 3)
    order = jax.random.permutation(order_key, lane_tally)
    lingering_shrinkage = order < lane_tally // 2
    slow_rate = jax.random.uniform(slow_key, (lane_tally,), jnp.float32, 0.1, 0.6) / LENGTH
    quick = fast_rate() * jnp.exp(jax.random.uniform(quick_key, (lane_tally,), jnp.float32, -0.35, 0.35))
    return (jnp.where(lingering_shrinkage, slow_rate, quick), lingering_shrinkage)


def sudden_line_selector(plain_quantity, lane_tally):
    place_key, depth_key = jax.random.split(plain_quantity, 2)
    places = jax.random.randint(place_key, (SEQS, lane_tally, 3), 0, LENGTH)
    depth = jnp.log(jax.random.uniform(depth_key, (SEQS, lane_tally, 3), jnp.float32, 0.5, 0.8))
    positions = jnp.arange(LENGTH)
    hits = positions[None, None, None, :] == places[..., None]
    return jnp.sum(jnp.where(hits, depth[..., None], 0.0), axis=2)


def drawn_pairs(key):
    plain_quantity = jax.random.fold_in(key, 7)
    query_key, keys_key = jax.random.split(plain_quantity, 2)
    queries = jnp.clip(jax.random.normal(query_key, (SEQS, LENGTH, FOX_QUESTIONERS * HEAD_DIM), jnp.float32), -6.0, 6.0)
    keys = jnp.clip(jax.random.normal(keys_key, (SEQS, LENGTH, KV_HEADS * HEAD_DIM), jnp.float32), -6.0, 6.0)
    return (queries.astype(jnp.bfloat16), keys.astype(jnp.bfloat16))


def draw_queries(key, part):
    return drawn_pairs(key)[0]


def draw_attention_keys(key, part):
    return drawn_pairs(key)[1]


def draw_forget_gate_cumsum(key, part):
    plain_quantity = jax.random.fold_in(key, 31)
    ratio_generator, portion_generator, sample_generator_start, sudden_generator = jax.random.split(plain_quantity, 4)
    shrinkage_ratios, lingering_shrinkage = head_rates(ratio_generator, FOX_QUESTIONERS)
    blocks = LENGTH // TOKENS_PER_SHARD
    stretch_coefficient = jnp.exp(jax.random.uniform(portion_generator, (SEQS, blocks, FOX_QUESTIONERS), jnp.float32, math.log(0.5), math.log(2.0)))
    stretch_coefficient = jnp.repeat(stretch_coefficient, TOKENS_PER_SHARD, axis=1)
    scatter_breadth = jnp.exp(0.7 * jnp.clip(jax.random.normal(sample_generator_start, (SEQS, LENGTH, FOX_QUESTIONERS), jnp.float32), -4.0, 4.0))
    sudden_arrivals = sudden_line_selector(sudden_generator, FOX_QUESTIONERS).transpose(0, 2, 1) * lingering_shrinkage.astype(jnp.float32)
    return jnp.cumsum(-shrinkage_ratios * stretch_coefficient * scatter_breadth + sudden_arrivals, axis=1)


def draw_lane_shrinkage_powers(key, part):
    shrinkage_ratios, _ = head_rates(jax.random.fold_in(key, 41), SPACE_MODEL_LANES)
    return jnp.log(shrinkage_ratios)


def draw_presoftplus_steps(key, part):
    plain_quantity = jax.random.fold_in(key, 47)
    offset_key, noise_key = jax.random.split(plain_quantity, 2)
    blocks = LENGTH // TOKENS_PER_SHARD
    offset = jax.random.uniform(offset_key, (SEQS, SPACE_MODEL_LANES, blocks), jnp.float32, -1.2, 1.2)
    offset = jnp.repeat(offset, TOKENS_PER_SHARD, axis=2)
    noise = jnp.clip(jax.random.normal(noise_key, (SEQS, SPACE_MODEL_LANES, LENGTH), jnp.float32), -4.0, 4.0)
    return offset + 0.8 * noise


def draw_extra_decay_log(key, part):
    return sudden_line_selector(jax.random.fold_in(key, 53), SPACE_MODEL_LANES)


def block_levels(key, extent, cuts, smallest, largest):
    def one(dim, blocks):
        draws = jax.random.uniform(jax.random.fold_in(jax.random.fold_in(key, 6), dim), (blocks,), jnp.float32, smallest / len(cuts), largest / len(cuts))
        return jnp.repeat(jnp.exp(draws), extent[dim] // blocks).reshape((-1,) + (1,) * (len(extent) - dim - 1))

    gain = one(*cuts[0])
    for cut in cuts[1:]:
        gain = gain * one(*cut)
    return gain


def gaussian(key, extent, scale, limit, cuts=(), held_as=jnp.bfloat16):
    gain = block_levels(key, extent, cuts, -0.22, 0.18) if cuts else 1.0
    drawn = jax.random.normal(key, extent, jnp.float32) * scale * gain
    return jnp.minimum(jnp.maximum(drawn, -limit), limit).astype(held_as)


def setup_inputs(seed: int = 0) -> dict:
    key_list = jax.random.split(jax.random.key(seed), 19)
    state_head_inputs = gaussian(key_list[0], (SEQS, LENGTH, SSD_WIDTH), 1.0, 6.0, ((0, 4), (1, 4), (2, 2)))
    state_write_vectors = gaussian(key_list[1], (SEQS, LENGTH, GROUPS * STATE), 0.5, 3.0, ((0, 4), (1, 4), (2, 2)))
    state_read_vectors = gaussian(key_list[2], (SEQS, LENGTH, GROUPS * STATE), 0.5, 3.0, ((0, 4), (1, 4), (2, 2)))
    state_output_gate = gaussian(key_list[3], (SEQS, LENGTH, SSD_WIDTH), 1.0, 6.0, ((0, 4), (1, 4), (2, 2)))
    presoftplus_steps = draw_presoftplus_steps(jax.random.fold_in(key_list[18], 71), 0)
    extra_decay_log = draw_extra_decay_log(jax.random.fold_in(key_list[18], 71), 0)
    lane_shrinkage_powers = draw_lane_shrinkage_powers(jax.random.fold_in(key_list[18], 71), 0)
    bypass_coefficient_vector = jnp.clip(jnp.exp(math.log(4.0) - 2.0794415 * jax.random.uniform(key_list[7], (SPACE_MODEL_LANES,), jnp.float32) ** block_levels(key_list[7], (SPACE_MODEL_LANES,), ((0, 2),), -0.2, 0.2)), 0.5, 4.0)
    feeder_smoothing_stencil = gaussian(key_list[8], (CONV, SSD_WIDTH), CONV ** -0.5, 3.0, ((1, 2),))
    stored_smoothing_stencil = gaussian(key_list[9], (CONV, GROUPS * STATE), CONV ** -0.5, 3.0, ((1, 2),))
    lookup_smoothing_stencil = gaussian(key_list[10], (CONV, GROUPS * STATE), CONV ** -0.5, 3.0, ((1, 2),))
    bundled_rescaling_vector = jnp.clip(1.0 + 0.18 * jax.random.normal(key_list[11], (SSD_WIDTH,), jnp.float32), 0.1, 1.9)
    queries = draw_queries(jax.random.fold_in(key_list[18], 71), 0)
    attention_keys = draw_attention_keys(jax.random.fold_in(key_list[18], 71), 0)
    attention_values = gaussian(key_list[14], (SEQS, LENGTH, KV_HEADS * HEAD_DIM), 1.0, 6.0, ((0, 4), (1, 4), (2, 2)))
    forget_gate_cumsum = draw_forget_gate_cumsum(jax.random.fold_in(key_list[18], 71), 0)
    state_out_weight = gaussian(key_list[16], (SSD_WIDTH, D), SSD_WIDTH ** -0.5, 0.1875, ((0, 2), (1, 4)))
    attention_out_weight = gaussian(key_list[17], (FOX_WIDTH, D), HEAD_DIM ** -0.5, 0.75, ((0, 2), (1, 4)))
    return {"state_head_inputs": state_head_inputs, "state_write_vectors": state_write_vectors, "state_read_vectors": state_read_vectors, "state_output_gate": state_output_gate, "presoftplus_steps": presoftplus_steps, "extra_decay_log": extra_decay_log, "lane_shrinkage_powers": lane_shrinkage_powers, "bypass_coefficient_vector": bypass_coefficient_vector, "feeder_smoothing_stencil": feeder_smoothing_stencil, "stored_smoothing_stencil": stored_smoothing_stencil, "lookup_smoothing_stencil": lookup_smoothing_stencil, "bundled_rescaling_vector": bundled_rescaling_vector, "queries": queries, "attention_keys": attention_keys, "attention_values": attention_values, "forget_gate_cumsum": forget_gate_cumsum, "state_out_weight": state_out_weight, "attention_out_weight": attention_out_weight}


EPSILON = 1e-06
NEGATIVE = -1e+30

def rounded_value(values):
    return lax.optimization_barrier(values.astype(jnp.bfloat16)).astype(jnp.float32)

def causal_filter(feeder_quantities, taps):
    length = feeder_quantities.shape[0]
    tap_count = taps.shape[0]
    padded = jnp.concatenate([jnp.zeros((tap_count - 1, feeder_quantities.shape[1]), jnp.float32), feeder_quantities.astype(jnp.float32)], axis=0)
    summed = jnp.zeros((length, feeder_quantities.shape[1]), jnp.float32)
    for offset in range(tap_count):
        summed = summed + taps[offset].astype(jnp.float32) * padded[offset:offset + length]
    return jax.nn.silu(summed).astype(jnp.bfloat16)

def memory_series_yield(feeder_quantities, stored_quantity, fetched_quantity, opening_quantity, bare_stride, sudden_arrivals, lane_shrinkage_powers, bypass_coefficient_vector, feeder_smoothing_stencil, stored_smoothing_stencil, lookup_smoothing_stencil, bundled_rescaling_vector):
    conv_values = causal_filter(feeder_quantities, feeder_smoothing_stencil)
    conv_write = causal_filter(stored_quantity, stored_smoothing_stencil)
    conv_read = causal_filter(fetched_quantity, lookup_smoothing_stencil)
    stride_duration = jax.nn.softplus(bare_stride)
    shrinkage_natural_power = stride_duration * (-jnp.exp(lane_shrinkage_powers))[:, None] + sudden_arrivals
    lane_tally = stride_duration.shape[0]
    per_group = lane_tally // GROUPS
    blocks = LENGTH // TOKENS_PER_SHARD
    positions = jnp.arange(TOKENS_PER_SHARD, dtype=jnp.int32)
    causal = positions[:, None] >= positions[None, :]

    def advance(carried, pieces):
        values, writes, reads, steps, decays = pieces
        cumulative = jnp.cumsum(decays, axis=1)
        input_heads = values.reshape(TOKENS_PER_SHARD, GROUPS, per_group, HEAD_DIM).astype(jnp.float32)
        write_groups = writes.reshape(TOKENS_PER_SHARD, GROUPS, STATE).astype(jnp.float32)
        read_groups = reads.reshape(TOKENS_PER_SHARD, GROUPS, STATE).astype(jnp.float32)
        inner_products = jnp.einsum('tgn,sgn->gts', read_groups, write_groups)
        log_gap = jnp.where(causal[None], cumulative[:, :, None] - cumulative[:, None, :], -jnp.inf)
        weights = jnp.exp(log_gap) * steps[:, None, :]
        mix_weights = rounded_value(inner_products[:, None] * weights.reshape(GROUPS, per_group, TOKENS_PER_SHARD, TOKENS_PER_SHARD))
        local_part = jnp.einsum('ghts,sghp->tghp', mix_weights, input_heads)
        end_scale = (jnp.exp(cumulative[:, -1:] - cumulative) * steps).T.reshape(TOKENS_PER_SHARD, GROUPS, per_group)
        weighted = rounded_value(input_heads * end_scale[..., None])
        block_state = jnp.einsum('sghp,sgn->ghpn', weighted, write_groups)
        total_decay = jnp.exp(cumulative[:, -1]).reshape(GROUPS, per_group)
        carried_part = jnp.einsum('tgn,ghpn->tghp', read_groups, rounded_value(carried))
        carried_part = carried_part * jnp.exp(cumulative).T.reshape(TOKENS_PER_SHARD, GROUPS, per_group)[..., None]
        mixer_sum = local_part + carried_part + bypass_coefficient_vector.reshape(GROUPS, per_group)[None, :, :, None] * input_heads
        following = total_decay[..., None, None] * carried + block_state
        return (following, mixer_sum)
    pieces = (conv_values.reshape(blocks, TOKENS_PER_SHARD, -1), conv_write.reshape(blocks, TOKENS_PER_SHARD, -1), conv_read.reshape(blocks, TOKENS_PER_SHARD, -1), stride_duration.reshape(lane_tally, blocks, TOKENS_PER_SHARD).transpose(1, 0, 2), shrinkage_natural_power.reshape(lane_tally, blocks, TOKENS_PER_SHARD).transpose(1, 0, 2))
    starting = jnp.zeros((GROUPS, per_group, HEAD_DIM, STATE), jnp.float32)
    _, sums = lax.scan(advance, starting, pieces)
    gated_rows = sums.reshape(LENGTH, GROUPS, per_group * HEAD_DIM) * jax.nn.silu(opening_quantity.astype(jnp.float32)).reshape(LENGTH, GROUPS, -1)
    stretch_coefficient = lax.rsqrt(lax.optimization_barrier(jnp.mean(gated_rows * gated_rows, axis=-1, keepdims=True)) + EPSILON)
    return (gated_rows * stretch_coefficient * bundled_rescaling_vector.reshape(GROUPS, -1)).reshape(LENGTH, -1).astype(jnp.bfloat16)

def attend_sequence(queries, keys, values, gates):
    blocks = LENGTH // TOKENS_PER_SHARD
    lane_tally = gates.shape[1]
    key_group_count = keys.shape[1] // HEAD_DIM
    repeat_factor = lane_tally // key_group_count
    query_blocks = queries.reshape(blocks, TOKENS_PER_SHARD, key_group_count, repeat_factor, HEAD_DIM)
    key_blocks = keys.reshape(blocks, TOKENS_PER_SHARD, key_group_count, HEAD_DIM)
    value_blocks = values.reshape(blocks, TOKENS_PER_SHARD, key_group_count, HEAD_DIM)
    gate_blocks = gates.reshape(blocks, TOKENS_PER_SHARD, lane_tally)
    attention_score_scale = HEAD_DIM ** (-0.5)

    def one_block(pieces):
        query_block, query_gates, block_index = pieces
        query_head_count = query_block.astype(jnp.float32)
        query_index = block_index * TOKENS_PER_SHARD + jnp.arange(TOKENS_PER_SHARD, dtype=jnp.int32)

        def advance(key_index, partial_value):
            running_max, running_sum, weighted_sum = partial_value
            key_tile = key_blocks[key_index].astype(jnp.float32)
            value_tile = value_blocks[key_index].astype(jnp.float32)
            key_gates = gate_blocks[key_index]
            attention_scores = jnp.einsum('ezxp,czp->zxec', query_head_count, key_tile).reshape(lane_tally, TOKENS_PER_SHARD, TOKENS_PER_SHARD) * attention_score_scale
            attention_scores = attention_scores + query_gates.T[:, :, None] - key_gates.T[:, None, :]
            key_place = key_index * TOKENS_PER_SHARD + jnp.arange(TOKENS_PER_SHARD, dtype=jnp.int32)
            visible = key_place[None, :] <= query_index[:, None]
            attention_scores = jnp.where(visible[None], attention_scores, NEGATIVE)
            new_max = jnp.maximum(running_max, lax.optimization_barrier(jnp.max(attention_scores, axis=-1)))
            shrink = jnp.exp(running_max - new_max)
            attention_probs = jnp.where(visible[None], jnp.exp(attention_scores - new_max[..., None]), 0.0)
            running_sum = running_sum * shrink + lax.optimization_barrier(jnp.sum(attention_probs, axis=-1))
            weighted_value_sum = jnp.einsum('fljx,xfc->fljc', rounded_value(attention_probs).reshape(key_group_count, repeat_factor, TOKENS_PER_SHARD, TOKENS_PER_SHARD), value_tile)
            weighted_sum = weighted_sum * shrink[..., None] + weighted_value_sum.reshape(lane_tally, TOKENS_PER_SHARD, HEAD_DIM)
            return (new_max, running_sum, weighted_sum)
        starting = (jnp.full((lane_tally, TOKENS_PER_SHARD), NEGATIVE, jnp.float32), jnp.zeros((lane_tally, TOKENS_PER_SHARD), jnp.float32), jnp.zeros((lane_tally, TOKENS_PER_SHARD, HEAD_DIM), jnp.float32))
        _, running_sum, weighted_sum = lax.fori_loop(0, block_index + 1, advance, starting)
        return (weighted_sum / running_sum[..., None]).transpose(1, 0, 2).reshape(TOKENS_PER_SHARD, -1).astype(jnp.bfloat16)
    outputs = lax.map(one_block, (query_blocks, gate_blocks, jnp.arange(blocks, dtype=jnp.int32)))
    return outputs.reshape(LENGTH, -1)

def reference(state_head_inputs, state_write_vectors, state_read_vectors, state_output_gate, presoftplus_steps, extra_decay_log, lane_shrinkage_powers, bypass_coefficient_vector, feeder_smoothing_stencil, stored_smoothing_stencil, lookup_smoothing_stencil, bundled_rescaling_vector, queries, attention_keys, attention_values, forget_gate_cumsum, state_out_weight, attention_out_weight):
    results = []
    for sequence_input in range(SEQS):
        state_result = memory_series_yield(state_head_inputs[sequence_input], state_write_vectors[sequence_input], state_read_vectors[sequence_input], state_output_gate[sequence_input], presoftplus_steps[sequence_input], extra_decay_log[sequence_input], lane_shrinkage_powers, bypass_coefficient_vector, feeder_smoothing_stencil, stored_smoothing_stencil, lookup_smoothing_stencil, bundled_rescaling_vector)
        attend_out = attend_sequence(queries[sequence_input], attention_keys[sequence_input], attention_values[sequence_input], forget_gate_cumsum[sequence_input])
        merged = jnp.dot(state_result, state_out_weight, preferred_element_type=jnp.float32) + jnp.dot(attend_out, attention_out_weight, preferred_element_type=jnp.float32)
        results.append(merged.astype(jnp.bfloat16))
    return jnp.stack(results)
```

```python
import functools
import math

import jax
import jax.numpy as jnp
from jax import lax
from jax.experimental import pallas as pl
from jax.experimental.pallas import tpu as pltpu
from jax.sharding import PartitionSpec as P

HEAD_DIM = 64
STATE = 128


EPSILON = 1e-06
NEGATIVE = -1e30


def passed_along(shard, axis, by):
    devices = lax.axis_size(axis)
    pairs = [(i, i + by) for i in range(devices) if 0 <= i + by < devices]
    return lax.ppermute(shard, axis, pairs)


def entering(shard, axis, join, neutral):
    place = lax.axis_index(axis)
    gathered = jax.tree.map(
        lambda a, kind: lax.all_gather(a.astype(kind), axis), shard, (jnp.bfloat16, jnp.bfloat16)
    )
    state = jax.tree.map(lambda a, e: jnp.zeros_like(a) + jnp.asarray(e, a.dtype), shard, neutral)

    def one(hop, state):
        return join(
            state,
            jax.tree.map(
                lambda a, own: lax.dynamic_index_in_dim(a, hop, 0, False).astype(own.dtype),
                gathered,
                shard,
            ),
        )

    return lax.fori_loop(0, place, one, state)


def causal_filter(feeder_quantities, before, taps):
    length = feeder_quantities.shape[0]
    padded = jnp.concatenate([before, feeder_quantities], axis=0).astype(jnp.float32)
    summed = jnp.zeros(feeder_quantities.shape, jnp.float32)
    for offset in range(taps.shape[0]):
        summed = summed + taps[offset].astype(jnp.float32) * padded[offset : offset + length]
    return jax.nn.silu(summed).astype(jnp.bfloat16)


def compose(earlier, later):
    return (earlier[0] * later[0], earlier[1] * later[0][..., None, None] + later[1])


def shards(
    state_head_inputs,
    state_write_vectors,
    state_read_vectors,
    state_output_gate,
    presoftplus_steps,
    extra_decay_log,
    lane_shrinkage_powers,
    bypass_coefficient_vector,
    feeder_smoothing_stencil,
    stored_smoothing_stencil,
    lookup_smoothing_stencil,
    bundled_rescaling_vector,
    queries,
    attention_keys,
    attention_values,
    forget_gate_cumsum,
    state_out_weight,
    attention_out_weight,
):
    shard_rows = state_head_inputs.shape[1]
    input_rows = state_head_inputs[0]
    write_rows = state_write_vectors[0]
    read_rows = state_read_vectors[0]
    tap_rows = feeder_smoothing_stencil.shape[0] - 1
    value_width = input_rows.shape[1]
    vector_width = write_rows.shape[1]
    tail_rows = jnp.concatenate(
        [input_rows[-tap_rows:], write_rows[-tap_rows:], read_rows[-tap_rows:]], axis=1
    )
    before = passed_along(tail_rows, "sp", 1)
    conv_values = causal_filter(input_rows, before[:, :value_width], feeder_smoothing_stencil)
    conv_write = causal_filter(
        write_rows, before[:, value_width : value_width + vector_width], stored_smoothing_stencil
    )
    conv_read = causal_filter(
        read_rows, before[:, value_width + vector_width :], lookup_smoothing_stencil
    )
    stride_duration = jax.nn.softplus(presoftplus_steps[0])
    shrinkage_natural_power = (
        stride_duration * (-jnp.exp(lane_shrinkage_powers))[:, None] + extra_decay_log[0]
    )
    lane_tally = stride_duration.shape[0]
    groups = vector_width // STATE
    per_group = lane_tally // groups
    cumulative = jnp.cumsum(shrinkage_natural_power, axis=1)
    input_heads = conv_values.reshape(shard_rows, groups, per_group, HEAD_DIM)
    write_groups = conv_write.reshape(shard_rows, groups, STATE)
    read_groups = conv_read.reshape(shard_rows, groups, STATE)
    inner_products = jnp.einsum(
        "tgn,sgn->gts", read_groups, write_groups, preferred_element_type=jnp.float32
    )
    positions = jnp.arange(shard_rows)
    causal = positions[:, None] >= positions[None, :]
    log_gap = jnp.where(causal[None], cumulative[:, :, None] - cumulative[:, None, :], -jnp.inf)
    weights = jnp.exp(log_gap) * stride_duration[:, None, :]
    mix_weights = (
        inner_products[:, None] * weights.reshape(groups, per_group, shard_rows, shard_rows)
    ).astype(jnp.bfloat16)
    local_part = jnp.einsum(
        "ghts,sghp->tghp", mix_weights, input_heads, preferred_element_type=jnp.float32
    )
    end_scale = (jnp.exp(cumulative[:, -1:] - cumulative) * stride_duration).T.reshape(
        shard_rows, groups, per_group
    )
    weighted = (input_heads.astype(jnp.float32) * end_scale[..., None]).astype(jnp.bfloat16)
    block_state = jnp.einsum(
        "sghp,sgn->ghpn", weighted, write_groups, preferred_element_type=jnp.float32
    )
    total_decay = jnp.exp(cumulative[:, -1]).reshape(groups, per_group)
    identity = (jnp.ones_like(total_decay), jnp.zeros_like(block_state))
    carried = entering((total_decay, block_state), "sp", compose, identity)[1]
    carried_part = jnp.einsum(
        "tgn,ghpn->tghp",
        read_groups,
        carried.astype(jnp.bfloat16),
        preferred_element_type=jnp.float32,
    )
    carried_part = (
        carried_part * jnp.exp(cumulative).T.reshape(shard_rows, groups, per_group)[..., None]
    )
    mixer_sum = (
        local_part
        + carried_part
        + bypass_coefficient_vector.reshape(groups, per_group)[None, :, :, None]
        * input_heads.astype(jnp.float32)
    )
    gated_rows = mixer_sum.reshape(shard_rows, groups, per_group * HEAD_DIM) * jax.nn.silu(
        state_output_gate[0].astype(jnp.float32)
    ).reshape(shard_rows, groups, -1)
    stretch_coefficient = lax.rsqrt(
        jnp.mean(gated_rows * gated_rows, axis=-1, keepdims=True) + EPSILON
    )
    state_result = (
        (gated_rows * stretch_coefficient * bundled_rescaling_vector.reshape(groups, -1))
        .reshape(shard_rows, -1)
        .astype(jnp.bfloat16)
    )
    attend_heads = forget_gate_cumsum.shape[2]
    key_group_count = attention_keys.shape[2] // HEAD_DIM
    repeat_factor = attend_heads // key_group_count
    query_head_count = queries[0].reshape(shard_rows, key_group_count, repeat_factor, HEAD_DIM)
    first_query = lax.axis_index("sp") * shard_rows
    query_index = first_query + jnp.arange(shard_rows)
    last_query = first_query + shard_rows - 1
    query_gates = forget_gate_cumsum[0].T
    all_gates = lax.all_gather(forget_gate_cumsum[0], "sp", axis=0, tiled=True)
    attention_score_scale = HEAD_DIM ** (-0.5)
    starting = (
        jnp.full((attend_heads, shard_rows), NEGATIVE, jnp.float32),
        jnp.zeros((attend_heads, shard_rows), jnp.float32),
        jnp.zeros((attend_heads, shard_rows, HEAD_DIM), jnp.float32),
    )
    key_rows = lax.all_gather(attention_keys[0], "sp", axis=0, tiled=True)
    value_rows = lax.all_gather(attention_values[0], "sp", axis=0, tiled=True)
    span = key_rows.shape[0]
    sub_block = math.gcd(span, 512)

    def advance(sub_index, running):
        first_key = sub_index * sub_block

        def attend(running):
            running_max, running_sum, weighted_sum = running
            key_tile = lax.dynamic_slice_in_dim(
                key_rows, sub_index * sub_block, sub_block, 0
            ).reshape(sub_block, key_group_count, HEAD_DIM)
            value_tile = lax.dynamic_slice_in_dim(
                value_rows, sub_index * sub_block, sub_block, 0
            ).reshape(sub_block, key_group_count, HEAD_DIM)
            key_gates = lax.dynamic_slice_in_dim(all_gates, first_key, sub_block, 0)
            attention_scores = jnp.einsum(
                "ezxp,czp->zxec", query_head_count, key_tile, preferred_element_type=jnp.float32
            )
            attention_scores = (
                attention_scores.reshape(attend_heads, shard_rows, sub_block)
                * attention_score_scale
            )
            attention_scores = attention_scores + query_gates[:, :, None] - key_gates.T[:, None, :]
            visible = (first_key + jnp.arange(sub_block))[None, :] <= query_index[:, None]
            attention_scores = jnp.where(visible[None], attention_scores, NEGATIVE)
            new_max = jnp.maximum(running_max, jnp.max(attention_scores, axis=-1))
            shrink = jnp.exp(running_max - new_max)
            attention_probs = jnp.where(
                visible[None], jnp.exp(attention_scores - new_max[..., None]), 0.0
            )
            running_sum = running_sum * shrink + jnp.sum(attention_probs, axis=-1)
            weighted_value_sum = jnp.einsum(
                "fljx,xfc->fljc",
                attention_probs.astype(jnp.bfloat16).reshape(
                    key_group_count, repeat_factor, shard_rows, sub_block
                ),
                value_tile,
                preferred_element_type=jnp.float32,
            )
            weighted_sum = weighted_sum * shrink[..., None] + weighted_value_sum.reshape(
                attend_heads, shard_rows, HEAD_DIM
            )
            return (new_max, running_sum, weighted_sum)

        return lax.cond(first_key <= last_query, attend, lambda kept: kept, running)

    _, running_sum, weighted_sum = lax.fori_loop(0, span // sub_block, advance, starting)
    attend_out = (
        (weighted_sum / running_sum[..., None])
        .transpose(1, 0, 2)
        .reshape(shard_rows, -1)
        .astype(jnp.bfloat16)
    )
    state_columns, attend_columns = (
        lax.all_gather(state_out_weight, "fs", axis=1, tiled=True),
        lax.all_gather(attention_out_weight, "fs", axis=1, tiled=True),
    )
    summed = lax.psum_scatter(
        (
            jnp.dot(state_result, state_columns, preferred_element_type=jnp.float32)
            + jnp.dot(attend_out, attend_columns, preferred_element_type=jnp.float32)
        ).astype(jnp.bfloat16),
        "tp",
        scatter_dimension=0,
        tiled=True,
    )
    return summed[None]


MESH = pl.DeviceIdType.MESH
LANES = 128
BF16, F32 = jnp.bfloat16, jnp.float32


def mixer_kernel(
    sp,
    fs,
    x_ref,
    w_ref,
    r_ref,
    gate_ref,
    step_ref,
    extra_ref,
    shrink_ref,
    bypass_ref,
    tapx_ref,
    tapw_ref,
    tapr_ref,
    gain_ref,
    q_ref,
    k_ref,
    v_ref,
    forget_ref,
    wst_ref,
    wat_ref,
    out_ref,
    pad_ref,
    tailx,
    tailw,
    tailr,
    kall,
    vall,
    gall,
    qs,
    states,
    decays,
    carried,
    mix,
    acts,
    acc,
    half_out,
    half_in,
    sums,
    landed,
    tail_send,
    tail_recv,
    kv_send,
    kv_recv,
    st_send,
    st_recv,
    act_send,
    act_recv,
    half_send,
    half_recv,
    sum_send,
    sum_recv,
):
    me = lax.axis_index("sp")
    f = lax.axis_index("fs")
    t = lax.axis_index("tp")
    rows, width = x_ref.shape[1], x_ref.shape[2]
    heads = step_ref.shape[1]
    kv_heads = k_ref.shape[2] // HEAD_DIM
    repeat = heads // kv_heads
    pairs = heads // 2
    taps = tapx_ref.shape[0]
    cols = wst_ref.shape[1]
    half = rows // 2

    barrier = pltpu.get_barrier_semaphore()
    for d in range(1, sp):
        pl.semaphore_signal(
            barrier, inc=1, device_id={"sp": lax.rem(me + d, sp)}, device_id_type=MESH
        )
    for d in range(1, fs):
        pl.semaphore_signal(
            barrier, inc=1, device_id={"fs": lax.rem(f + d, fs)}, device_id_type=MESH
        )
    pl.semaphore_signal(barrier, inc=1, device_id={"tp": 1 - t}, device_id_type=MESH)

    def remote(src, dst, send, recv, where):
        return pltpu.make_async_remote_copy(
            src_ref=src,
            dst_ref=dst,
            send_sem=send,
            recv_sem=recv,
            device_id=where,
            device_id_type=MESH,
        )

    gall[me] = forget_ref[0].T
    kall[me] = k_ref[0]
    vall[me] = v_ref[0]
    pl.semaphore_wait(barrier, sp - 1 + fs - 1 + 1)

    tail = [
        remote(
            src.at[0, rows - 16 : rows, :],
            dst,
            tail_send.at[i],
            tail_recv.at[i],
            {"sp": lax.rem(me + 1, sp)},
        )
        for i, (src, dst) in enumerate(((x_ref, tailx), (w_ref, tailw), (r_ref, tailr)))
    ]

    @pl.when(me < sp - 1)
    def _():
        for copy in tail:
            copy.start()

    def kv_copies(d, source):
        there = {"sp": lax.rem(me + d, sp)}
        return [
            remote(src, dst.at[source], kv_send.at[d, i], kv_recv.at[source, i], there)
            for i, (src, dst) in enumerate(
                ((k_ref.at[0], kall), (v_ref.at[0], vall), (gall.at[me], gall))
            )
        ]

    for d in range(1, sp):

        @pl.when(me + d < sp)
        def _(d=d):
            for copy in kv_copies(d, me):
                copy.start()

    lane = lax.broadcasted_iota(jnp.int32, (1, LANES), 1)
    low = lane < HEAD_DIM
    row_id = lax.broadcasted_iota(jnp.int32, (rows, rows), 0)
    col_id = lax.broadcasted_iota(jnp.int32, (rows, rows), 1)

    for j in range(1, sp):

        @pl.when(j > me)
        def _(j=j):
            kall[j] = jnp.zeros(kall.shape[1:], BF16)
            vall[j] = jnp.zeros(vall.shape[1:], BF16)
            gall[j] = jnp.zeros(gall.shape[1:], F32)

    for h in range(heads):
        kv = h // repeat
        piece = (q_ref[0, :, h * HEAD_DIM : (h + 1) * HEAD_DIM].astype(F32) * HEAD_DIM**-0.5).astype(
            BF16
        )
        zero = jnp.zeros((rows, HEAD_DIM), BF16)
        parts = [piece if i == kv else zero for i in range(kv_heads)]
        qs[kv, (h % repeat) * rows : (h % repeat + 1) * rows, :] = jnp.concatenate(parts, axis=1)

    head_row = lax.broadcasted_iota(jnp.int32, (heads, rows), 0)
    power = jnp.zeros((heads, rows), F32)
    for h in range(heads):
        power = jnp.where(head_row == h, shrink_ref[h], power)
    presoft = step_ref[0]
    step = jnp.maximum(presoft, 0.0) + jnp.log1p(jnp.exp(-jnp.abs(presoft)))
    log_decay = extra_ref[0] - jnp.exp(power) * step
    upper = (row_id <= col_id).astype(F32)
    cum = jnp.dot(log_decay, upper, precision=lax.Precision.HIGHEST, preferred_element_type=F32)
    cum_end = cum[:, rows - 1 : rows]
    end_scale = (jnp.exp(cum_end - cum) * step).T
    exp_cum = jnp.exp(cum).T
    cum_col = cum.T
    decays[me] = jnp.broadcast_to(jnp.exp(cum_end), (heads, LANES))

    @pl.when(me > 0)
    def _():
        for copy in tail:
            copy.wait_recv()

    def filtered(ref, tail_ref, tap_ref, n):
        before = jnp.where(me > 0, tail_ref[...].astype(F32)[8:16], 0.0)
        pad_ref[0:8, 0:n] = before
        pad_ref[8 : 8 + rows, 0:n] = ref[0].astype(F32)
        total = jnp.zeros((rows, n), F32)
        for i in range(taps):
            at = 8 - (taps - 1) + i
            total = total + tap_ref[i : i + 1, :].astype(F32) * pad_ref[at : at + rows, 0:n]
        return (total * jax.nn.sigmoid(total)).astype(BF16)

    conv_write = filtered(w_ref, tailw, tapw_ref, STATE)
    conv_values = filtered(x_ref, tailx, tapx_ref, width)

    def expand(columns, j):
        return jnp.where(low, columns[:, 2 * j : 2 * j + 1], columns[:, 2 * j + 1 : 2 * j + 2])

    weighted = jnp.concatenate(
        [
            (
                conv_values[:, j * LANES : (j + 1) * LANES].astype(F32) * expand(end_scale, j)
            ).astype(BF16)
            for j in range(pairs)
        ],
        axis=1,
    )
    states[me] = lax.dot_general(
        conv_write, weighted, (((0,), (0,)), ((), ())), preferred_element_type=F32
    ).astype(BF16)

    def st_copies(d, source):
        there = {"sp": lax.rem(me + d, sp)}
        return [
            remote(buf.at[source], buf.at[source], st_send.at[d, i], st_recv.at[source, i], there)
            for i, buf in enumerate((states, decays))
        ]

    for d in range(1, sp):

        @pl.when(me + d < sp)
        def _(d=d):
            for copy in st_copies(d, me):
                copy.start()

    conv_read = filtered(r_ref, tailr, tapr_ref, STATE)
    inner = lax.dot_general(
        conv_read, conv_write, (((1,), (1,)), ((), ())), preferred_element_type=F32
    )
    causal = row_id >= col_id
    for j in range(pairs):
        tile = conv_values[:, j * LANES : (j + 1) * LANES]
        parts = []
        for h in (2 * j, 2 * j + 1):
            gap = jnp.where(causal, cum_col[:, h : h + 1] - cum[h : h + 1, :], NEGATIVE)
            weights = (inner * (jnp.exp(gap) * step[h : h + 1, :])).astype(BF16)
            parts.append(jnp.dot(weights, tile, preferred_element_type=F32))
        bypass = jnp.where(low, bypass_ref[2 * j], bypass_ref[2 * j + 1])
        mix[:, j * LANES : (j + 1) * LANES] = (
            jnp.where(low, parts[0], parts[1]) + bypass * tile.astype(F32)
        )

    for j in range(sp - 1):

        @pl.when(j < me)
        def _(j=j):
            for copy in kv_copies(1, j):
                copy.wait_recv()

    keys = kall[...].reshape(sp * rows, -1)
    values = vall[...].reshape(sp * rows, -1)
    visible = [j * rows + col_id <= me * rows + row_id for j in range(sp)]
    for kv in range(kv_heads):
        own = lane // HEAD_DIM == kv
        summed_values = jnp.where(own, values, jnp.ones_like(values))
        scores = lax.dot_general(
            qs[kv], keys, (((1,), (1,)), ((), ())), preferred_element_type=F32
        )
        outs = []
        for i in range(repeat):
            h = kv * repeat + i
            gate_col = forget_ref[0, :, h : h + 1]
            tiles = [
                jnp.where(
                    visible[j],
                    scores[i * rows : (i + 1) * rows, j * rows : (j + 1) * rows]
                    + (gate_col - gall[j, h : h + 1, :]),
                    NEGATIVE,
                )
                for j in range(sp)
            ]
            top = tiles[0]
            for tile in tiles[1:]:
                top = jnp.maximum(top, tile)
            top = jnp.max(top, axis=1, keepdims=True)
            probs = jnp.concatenate([jnp.exp(tile - top).astype(BF16) for tile in tiles], axis=1)
            both = jnp.dot(probs, summed_values, preferred_element_type=F32)
            turned = pltpu.roll(both, HEAD_DIM, 1)
            outs.append(both / turned if h % 2 == kv else turned / both)
        for i in range(0, repeat, 2):
            h = kv * repeat + i
            acts[0, 0, :, h * HEAD_DIM : (h + 2) * HEAD_DIM] = jnp.where(
                low, outs[i], outs[i + 1]
            ).astype(BF16)

    def act_copy(kind, origin, hop):
        return remote(
            acts.at[kind, origin],
            acts.at[kind, origin ^ hop],
            act_send.at[kind, origin ^ hop],
            act_recv.at[kind, origin ^ hop],
            {"fs": lax.rem(f + 0, fs) ^ hop},
        )

    act_copy(0, 0, 1).start()
    act_copy(0, 0, 2).start()
    acc[0] = jnp.dot(acts[0, 0], wat_ref[...], preferred_element_type=F32)
    act_copy(0, 0, 1).wait_recv()
    act_copy(0, 1, 2).start()
    acc[1] = jnp.dot(acts[0, 1], wat_ref[...], preferred_element_type=F32)

    carried[...] = jnp.zeros(carried.shape, F32)
    for j in range(sp - 1):

        @pl.when(j < me)
        def _(j=j):
            for copy in st_copies(1, j):
                copy.wait_recv()
            for p in range(pairs):
                at = slice(p * LANES, (p + 1) * LANES)
                decay = jnp.where(
                    low, decays[j, 2 * p : 2 * p + 1, :], decays[j, 2 * p + 1 : 2 * p + 2, :]
                )
                carried[:, at] = carried[:, at] * decay + states[j, :, at].astype(F32)

    entered = jnp.dot(conv_read, carried[...].astype(BF16), preferred_element_type=F32)
    squares = jnp.zeros((rows, LANES), F32)
    gated = []
    for p in range(pairs):
        at = slice(p * LANES, (p + 1) * LANES)
        gate = gate_ref[0, :, at].astype(F32)
        u = (mix[:, at] + entered[:, at] * expand(exp_cum, p)) * (gate * jax.nn.sigmoid(gate))
        gated.append(u)
        squares = squares + u * u
    scale = lax.rsqrt(jnp.sum(squares, axis=1, keepdims=True) / width + EPSILON)
    for p in range(pairs):
        at = slice(p * LANES, (p + 1) * LANES)
        acts[1, 0, :, at] = (gated[p] * scale * gain_ref[0:1, at]).astype(BF16)
    act_copy(1, 0, 2).start()
    act_copy(1, 0, 1).start()

    def half_copy(d):
        return remote(
            half_out.at[d], half_in.at[d], half_send.at[d], half_recv.at[d], {"tp": 1 - t}
        )

    def give(d):
        there = pl.ds(pl.multiple_of((1 - t) * half, half), half)
        half_out[d] = acc[d, there, :].astype(BF16)
        half_copy(d).start()

    def sum_copy(d):
        return remote(sums.at[d], landed.at[d], sum_send.at[d], sum_recv.at[d], {"fs": f ^ d})

    def finish(d):
        half_copy(d).wait_recv()
        here = pl.ds(pl.multiple_of(t * half, half), half)
        total = (acc[d, here, :] + half_in[d].astype(F32)).astype(BF16)
        if d:
            sums[d] = total
            sum_copy(d).start()
        else:
            out_ref[0, :, pl.ds(pl.multiple_of(f * cols, cols), cols)] = total

    acc[0] += jnp.dot(acts[1, 0], wst_ref[...], preferred_element_type=F32)
    give(0)
    act_copy(0, 0, 2).wait_recv()
    acc[2] = jnp.dot(acts[0, 2], wat_ref[...], preferred_element_type=F32)
    act_copy(0, 1, 2).wait_recv()
    acc[3] = jnp.dot(acts[0, 3], wat_ref[...], preferred_element_type=F32)
    act_copy(1, 0, 2).wait_recv()
    act_copy(1, 2, 1).start()
    acc[2] += jnp.dot(acts[1, 2], wst_ref[...], preferred_element_type=F32)
    give(2)
    act_copy(1, 0, 1).wait_recv()
    acc[1] += jnp.dot(acts[1, 1], wst_ref[...], preferred_element_type=F32)
    give(1)
    finish(0)
    finish(2)
    finish(1)
    act_copy(1, 2, 1).wait_recv()
    acc[3] += jnp.dot(acts[1, 3], wst_ref[...], preferred_element_type=F32)
    give(3)
    finish(3)
    for d in (2, 1, 3):
        sum_copy(d).wait_recv()
        out_ref[0, :, pl.ds(pl.multiple_of((f ^ d) * cols, cols), cols)] = landed[d]

    @pl.when(me < sp - 1)
    def _():
        for copy in tail:
            copy.wait_send()

    for d in range(1, sp):

        @pl.when(me + d < sp)
        def _(d=d):
            for copy in kv_copies(d, me) + st_copies(d, me):
                copy.wait_send()

    for kind, via in ((0, 1), (1, 2)):
        act_copy(kind, 0, 1).wait_send()
        act_copy(kind, 0, 2).wait_send()
        act_copy(kind, via, 3 ^ via).wait_send()
    for d in range(fs):
        half_copy(d).wait_send()
    for d in range(1, fs):
        sum_copy(d).wait_send()


def fused(sp, fs, *args):
    x, w = args[0], args[1]
    rows, width = x.shape[1], x.shape[2]
    heads = args[4].shape[1]
    cols = args[16].shape[1]
    half = rows // 2
    args = list(args)
    args[11] = args[11].reshape(1, -1)
    vmem = pl.BlockSpec(memory_space=pltpu.VMEM)
    smem = pl.BlockSpec(memory_space=pltpu.SMEM)
    specs = [smem if i in (6, 7) else vmem for i in range(len(args))]
    dma = pltpu.SemaphoreType.DMA
    kv_width = args[13].shape[2]
    kv_heads = kv_width // HEAD_DIM
    return pl.pallas_call(
        functools.partial(mixer_kernel, sp, fs),
        out_shape=jax.ShapeDtypeStruct((1, half, cols * fs), BF16),
        in_specs=specs,
        out_specs=vmem,
        scratch_shapes=[
            pltpu.VMEM((8 + rows, width), F32),
            pltpu.VMEM((16, width), BF16),
            pltpu.VMEM((16, w.shape[2]), BF16),
            pltpu.VMEM((16, w.shape[2]), BF16),
            pltpu.VMEM((sp, rows, kv_width), BF16),
            pltpu.VMEM((sp, rows, kv_width), BF16),
            pltpu.VMEM((sp, heads, rows), F32),
            pltpu.VMEM((kv_heads, heads // kv_heads * rows, kv_width), BF16),
            pltpu.VMEM((sp, STATE, width), BF16),
            pltpu.VMEM((sp, heads, LANES), F32),
            pltpu.VMEM((STATE, width), F32),
            pltpu.VMEM((rows, width), F32),
            pltpu.VMEM((2, fs, rows, width), BF16),
            pltpu.VMEM((fs, rows, cols), F32),
            pltpu.VMEM((fs, half, cols), BF16),
            pltpu.VMEM((fs, half, cols), BF16),
            pltpu.VMEM((fs, half, cols), BF16),
            pltpu.VMEM((fs, half, cols), BF16),
            dma((3,)),
            dma((3,)),
            dma((sp, 3)),
            dma((sp, 3)),
            dma((sp, 2)),
            dma((sp, 2)),
            dma((2, fs)),
            dma((2, fs)),
            dma((fs,)),
            dma((fs,)),
            dma((fs,)),
            dma((fs,)),
        ],
        compiler_params=pltpu.CompilerParams(collective_id=0, has_side_effects=True),
    )(*args)


def one_kernel(*args, sp, fs, tp):
    rows, width = args[0].shape[1:]
    heads = args[4].shape[1]
    return (
        1 < sp <= 8
        and fs == 4
        and tp == 2
        and rows == LANES
        and args[1].shape[2] == STATE
        and width == heads * HEAD_DIM
        and args[12].shape[2] == width
        and args[13].shape[2] == 2 * HEAD_DIM
        and heads % 4 == 0
    )


def solution(mesh):
    in_specs = (
        P("fs", "sp", "tp"),
        P("fs", "sp", "tp"),
        P("fs", "sp", "tp"),
        P("fs", "sp", "tp"),
        P("fs", "tp", "sp"),
        P("fs", "tp", "sp"),
        P("tp"),
        P("tp"),
        P(None, "tp"),
        P(None, "tp"),
        P(None, "tp"),
        P("tp"),
        P("fs", "sp", "tp"),
        P("fs", "sp", "tp"),
        P("fs", "sp", "tp"),
        P("fs", "sp", "tp"),
        P("tp", "fs"),
        P("tp", "fs"),
    )
    out_specs = P("fs", ("sp", "tp"), None)
    sp, fs, tp = (mesh.shape[name] for name in ("sp", "fs", "tp"))

    def body(*args):
        if one_kernel(*args, sp=sp, fs=fs, tp=tp):
            return fused(sp, fs, *args)
        return shards(*args)

    return jax.shard_map(body, mesh=mesh, in_specs=in_specs, out_specs=out_specs, check_vma=False)
```

```python
import functools
import math

import jax
import jax.numpy as jnp
from jax import lax
from jax.experimental import pallas as pl
from jax.experimental.pallas import tpu as pltpu
from jax.sharding import PartitionSpec as P

HEAD_DIM = 64
STATE = 128


EPSILON = 1e-06
NEGATIVE = -1e30


def passed_along(shard, axis, by):
    devices = lax.axis_size(axis)
    pairs = [(i, i + by) for i in range(devices) if 0 <= i + by < devices]
    return lax.ppermute(shard, axis, pairs)


def entering(shard, axis, join, neutral):
    place = lax.axis_index(axis)
    gathered = jax.tree.map(
        lambda a, kind: lax.all_gather(a.astype(kind), axis), shard, (jnp.bfloat16, jnp.bfloat16)
    )
    state = jax.tree.map(lambda a, e: jnp.zeros_like(a) + jnp.asarray(e, a.dtype), shard, neutral)

    def one(hop, state):
        return join(
            state,
            jax.tree.map(
                lambda a, own: lax.dynamic_index_in_dim(a, hop, 0, False).astype(own.dtype),
                gathered,
                shard,
            ),
        )

    return lax.fori_loop(0, place, one, state)


def causal_filter(feeder_quantities, before, taps):
    length = feeder_quantities.shape[0]
    padded = jnp.concatenate([before, feeder_quantities], axis=0).astype(jnp.float32)
    summed = jnp.zeros(feeder_quantities.shape, jnp.float32)
    for offset in range(taps.shape[0]):
        summed = summed + taps[offset].astype(jnp.float32) * padded[offset : offset + length]
    return jax.nn.silu(summed).astype(jnp.bfloat16)


def compose(earlier, later):
    return (earlier[0] * later[0], earlier[1] * later[0][..., None, None] + later[1])


def shards(
    state_head_inputs,
    state_write_vectors,
    state_read_vectors,
    state_output_gate,
    presoftplus_steps,
    extra_decay_log,
    lane_shrinkage_powers,
    bypass_coefficient_vector,
    feeder_smoothing_stencil,
    stored_smoothing_stencil,
    lookup_smoothing_stencil,
    bundled_rescaling_vector,
    queries,
    attention_keys,
    attention_values,
    forget_gate_cumsum,
    state_out_weight,
    attention_out_weight,
):
    shard_rows = state_head_inputs.shape[1]
    input_rows = state_head_inputs[0]
    write_rows = state_write_vectors[0]
    read_rows = state_read_vectors[0]
    tap_rows = feeder_smoothing_stencil.shape[0] - 1
    value_width = input_rows.shape[1]
    vector_width = write_rows.shape[1]
    tail_rows = jnp.concatenate(
        [input_rows[-tap_rows:], write_rows[-tap_rows:], read_rows[-tap_rows:]], axis=1
    )
    before = passed_along(tail_rows, "sp", 1)
    conv_values = causal_filter(input_rows, before[:, :value_width], feeder_smoothing_stencil)
    conv_write = causal_filter(
        write_rows, before[:, value_width : value_width + vector_width], stored_smoothing_stencil
    )
    conv_read = causal_filter(
        read_rows, before[:, value_width + vector_width :], lookup_smoothing_stencil
    )
    stride_duration = jax.nn.softplus(presoftplus_steps[0])
    shrinkage_natural_power = (
        stride_duration * (-jnp.exp(lane_shrinkage_powers))[:, None] + extra_decay_log[0]
    )
    lane_tally = stride_duration.shape[0]
    groups = vector_width // STATE
    per_group = lane_tally // groups
    cumulative = jnp.cumsum(shrinkage_natural_power, axis=1)
    input_heads = conv_values.reshape(shard_rows, groups, per_group, HEAD_DIM)
    write_groups = conv_write.reshape(shard_rows, groups, STATE)
    read_groups = conv_read.reshape(shard_rows, groups, STATE)
    inner_products = jnp.einsum(
        "tgn,sgn->gts", read_groups, write_groups, preferred_element_type=jnp.float32
    )
    positions = jnp.arange(shard_rows)
    causal = positions[:, None] >= positions[None, :]
    log_gap = jnp.where(causal[None], cumulative[:, :, None] - cumulative[:, None, :], -jnp.inf)
    weights = jnp.exp(log_gap) * stride_duration[:, None, :]
    mix_weights = (
        inner_products[:, None] * weights.reshape(groups, per_group, shard_rows, shard_rows)
    ).astype(jnp.bfloat16)
    local_part = jnp.einsum(
        "ghts,sghp->tghp", mix_weights, input_heads, preferred_element_type=jnp.float32
    )
    end_scale = (jnp.exp(cumulative[:, -1:] - cumulative) * stride_duration).T.reshape(
        shard_rows, groups, per_group
    )
    weighted = (input_heads.astype(jnp.float32) * end_scale[..., None]).astype(jnp.bfloat16)
    block_state = jnp.einsum(
        "sghp,sgn->ghpn", weighted, write_groups, preferred_element_type=jnp.float32
    )
    total_decay = jnp.exp(cumulative[:, -1]).reshape(groups, per_group)
    identity = (jnp.ones_like(total_decay), jnp.zeros_like(block_state))
    carried = entering((total_decay, block_state), "sp", compose, identity)[1]
    carried_part = jnp.einsum(
        "tgn,ghpn->tghp",
        read_groups,
        carried.astype(jnp.bfloat16),
        preferred_element_type=jnp.float32,
    )
    carried_part = (
        carried_part * jnp.exp(cumulative).T.reshape(shard_rows, groups, per_group)[..., None]
    )
    mixer_sum = (
        local_part
        + carried_part
        + bypass_coefficient_vector.reshape(groups, per_group)[None, :, :, None]
        * input_heads.astype(jnp.float32)
    )
    gated_rows = mixer_sum.reshape(shard_rows, groups, per_group * HEAD_DIM) * jax.nn.silu(
        state_output_gate[0].astype(jnp.float32)
    ).reshape(shard_rows, groups, -1)
    stretch_coefficient = lax.rsqrt(
        jnp.mean(gated_rows * gated_rows, axis=-1, keepdims=True) + EPSILON
    )
    state_result = (
        (gated_rows * stretch_coefficient * bundled_rescaling_vector.reshape(groups, -1))
        .reshape(shard_rows, -1)
        .astype(jnp.bfloat16)
    )
    attend_heads = forget_gate_cumsum.shape[2]
    key_group_count = attention_keys.shape[2] // HEAD_DIM
    repeat_factor = attend_heads // key_group_count
    query_head_count = queries[0].reshape(shard_rows, key_group_count, repeat_factor, HEAD_DIM)
    first_query = lax.axis_index("sp") * shard_rows
    query_index = first_query + jnp.arange(shard_rows)
    last_query = first_query + shard_rows - 1
    query_gates = forget_gate_cumsum[0].T
    all_gates = lax.all_gather(forget_gate_cumsum[0], "sp", axis=0, tiled=True)
    attention_score_scale = HEAD_DIM ** (-0.5)
    starting = (
        jnp.full((attend_heads, shard_rows), NEGATIVE, jnp.float32),
        jnp.zeros((attend_heads, shard_rows), jnp.float32),
        jnp.zeros((attend_heads, shard_rows, HEAD_DIM), jnp.float32),
    )
    key_rows = lax.all_gather(attention_keys[0], "sp", axis=0, tiled=True)
    value_rows = lax.all_gather(attention_values[0], "sp", axis=0, tiled=True)
    span = key_rows.shape[0]
    sub_block = math.gcd(span, 512)

    def advance(sub_index, running):
        first_key = sub_index * sub_block

        def attend(running):
            running_max, running_sum, weighted_sum = running
            key_tile = lax.dynamic_slice_in_dim(
                key_rows, sub_index * sub_block, sub_block, 0
            ).reshape(sub_block, key_group_count, HEAD_DIM)
            value_tile = lax.dynamic_slice_in_dim(
                value_rows, sub_index * sub_block, sub_block, 0
            ).reshape(sub_block, key_group_count, HEAD_DIM)
            key_gates = lax.dynamic_slice_in_dim(all_gates, first_key, sub_block, 0)
            attention_scores = jnp.einsum(
                "ezxp,czp->zxec", query_head_count, key_tile, preferred_element_type=jnp.float32
            )
            attention_scores = (
                attention_scores.reshape(attend_heads, shard_rows, sub_block)
                * attention_score_scale
            )
            attention_scores = attention_scores + query_gates[:, :, None] - key_gates.T[:, None, :]
            visible = (first_key + jnp.arange(sub_block))[None, :] <= query_index[:, None]
            attention_scores = jnp.where(visible[None], attention_scores, NEGATIVE)
            new_max = jnp.maximum(running_max, jnp.max(attention_scores, axis=-1))
            shrink = jnp.exp(running_max - new_max)
            attention_probs = jnp.where(
                visible[None], jnp.exp(attention_scores - new_max[..., None]), 0.0
            )
            running_sum = running_sum * shrink + jnp.sum(attention_probs, axis=-1)
            weighted_value_sum = jnp.einsum(
                "fljx,xfc->fljc",
                attention_probs.astype(jnp.bfloat16).reshape(
                    key_group_count, repeat_factor, shard_rows, sub_block
                ),
                value_tile,
                preferred_element_type=jnp.float32,
            )
            weighted_sum = weighted_sum * shrink[..., None] + weighted_value_sum.reshape(
                attend_heads, shard_rows, HEAD_DIM
            )
            return (new_max, running_sum, weighted_sum)

        return lax.cond(first_key <= last_query, attend, lambda kept: kept, running)

    _, running_sum, weighted_sum = lax.fori_loop(0, span // sub_block, advance, starting)
    attend_out = (
        (weighted_sum / running_sum[..., None])
        .transpose(1, 0, 2)
        .reshape(shard_rows, -1)
        .astype(jnp.bfloat16)
    )
    state_columns, attend_columns = (
        lax.all_gather(state_out_weight, "fs", axis=1, tiled=True),
        lax.all_gather(attention_out_weight, "fs", axis=1, tiled=True),
    )
    summed = lax.psum_scatter(
        (
            jnp.dot(state_result, state_columns, preferred_element_type=jnp.float32)
            + jnp.dot(attend_out, attend_columns, preferred_element_type=jnp.float32)
        ).astype(jnp.bfloat16),
        "tp",
        scatter_dimension=0,
        tiled=True,
    )
    return summed[None]


MESH = pl.DeviceIdType.MESH
LANES = 128
BF16, F32 = jnp.bfloat16, jnp.float32


def mixer_kernel(
    sp,
    fs,
    x_ref,
    w_ref,
    r_ref,
    gate_ref,
    step_ref,
    extra_ref,
    shrink_ref,
    bypass_ref,
    tapx_ref,
    tapw_ref,
    tapr_ref,
    gain_ref,
    q_ref,
    k_ref,
    v_ref,
    forget_ref,
    wst_ref,
    wat_ref,
    out_ref,
    pad_ref,
    tails,
    conv,
    end_wide,
    kall,
    vall,
    gall,
    qs,
    states,
    decays,
    carried,
    mix,
    acts,
    pieces,
    scales,
    acc,
    acc_state,
    half_out,
    half_in,
    sums,
    landed,
    tail_send,
    tail_recv,
    kv_send,
    kv_recv,
    st_send,
    st_recv,
    act_send,
    act_recv,
    piece_send,
    piece_recv,
    half_send,
    half_recv,
    sum_send,
    sum_recv,
):
    me = lax.axis_index("sp")
    f = lax.axis_index("fs")
    t = lax.axis_index("tp")
    rows, width = x_ref.shape[1], x_ref.shape[2]
    heads = step_ref.shape[1]
    kv_heads = k_ref.shape[2] // HEAD_DIM
    repeat = heads // kv_heads
    pairs = heads // 2
    taps = tapx_ref.shape[0]
    cols = wst_ref.shape[1]
    half = rows // 2

    barrier = pltpu.get_barrier_semaphore()
    for d in range(1, sp):
        pl.semaphore_signal(
            barrier, inc=1, device_id={"sp": lax.rem(me + d, sp)}, device_id_type=MESH
        )
    for d in range(1, fs):
        pl.semaphore_signal(
            barrier, inc=1, device_id={"fs": lax.rem(f + d, fs)}, device_id_type=MESH
        )
    pl.semaphore_signal(barrier, inc=1, device_id={"tp": 1 - t}, device_id_type=MESH)

    def remote(src, dst, send, recv, where):
        return pltpu.make_async_remote_copy(
            src_ref=src,
            dst_ref=dst,
            send_sem=send,
            recv_sem=recv,
            device_id=where,
            device_id_type=MESH,
        )

    lane = lax.broadcasted_iota(jnp.int32, (1, LANES), 1)
    low = lane < HEAD_DIM
    row_id = lax.broadcasted_iota(jnp.int32, (rows, rows), 0)
    col_id = lax.broadcasted_iota(jnp.int32, (rows, rows), 1)

    def expand(columns, j):
        return jnp.where(low, columns[:, 2 * j : 2 * j + 1], columns[:, 2 * j + 1 : 2 * j + 2])

    gall[me] = forget_ref[0]
    gate_cols = forget_ref[0].T
    kall[me] = k_ref[0]
    vall[me] = v_ref[0]

    inputs = (
        (x_ref, tapx_ref, slice(0, width)),
        (w_ref, tapw_ref, slice(width, width + STATE)),
        (r_ref, tapr_ref, slice(width + STATE, width + 2 * STATE)),
    )

    def filtered(count):
        for _, tap_ref, at in inputs:
            total = jnp.zeros((count, at.stop - at.start), F32)
            for i in range(taps):
                first = 8 - (taps - 1) + i
                total = total + tap_ref[i : i + 1, :].astype(F32) * pad_ref[first : first + count, at]
            conv[0:count, at] = (total * jax.nn.sigmoid(total)).astype(BF16)

    pad_ref[0:8, :] = jnp.zeros((8, pad_ref.shape[1]), F32)
    for ref, _, at in inputs:
        pad_ref[8 : 8 + rows, at] = ref[0].astype(F32)
    filtered(rows)

    head_row = lax.broadcasted_iota(jnp.int32, (heads, rows), 0)
    power = jnp.zeros((heads, rows), F32)
    for h in range(heads):
        power = jnp.where(head_row == h, shrink_ref[h], power)
    presoft = step_ref[0]
    step = jnp.maximum(presoft, 0.0) + jnp.log1p(jnp.exp(-jnp.abs(presoft)))
    log_decay = extra_ref[0] - jnp.exp(power) * step
    upper = (row_id <= col_id).astype(F32)
    cum = jnp.dot(log_decay, upper, precision=lax.Precision.HIGHEST, preferred_element_type=F32)
    cum_end = cum[:, rows - 1 : rows]
    decays[me] = jnp.broadcast_to(jnp.exp(cum_end), (heads, LANES))
    end_scale = (jnp.exp(cum_end - cum) * step).T
    for j in range(pairs):
        end_wide[:, j * LANES : (j + 1) * LANES] = expand(end_scale, j)

    pl.semaphore_wait(barrier, sp - 1 + fs - 1 + 1)

    tail = [
        remote(
            ref.at[0, rows - 16 : rows, :],
            tails.at[:, at],
            tail_send.at[i],
            tail_recv.at[i],
            {"sp": lax.rem(me + 1, sp)},
        )
        for i, (ref, _, at) in enumerate(inputs)
    ]

    @pl.when(me < sp - 1)
    def _():
        for copy in tail:
            copy.start()

    def kv_copies(d, source):
        there = {"sp": lax.rem(me + d, sp)}
        return [
            remote(src, dst.at[source], kv_send.at[d, i], kv_recv.at[source, i], there)
            for i, (src, dst) in enumerate(
                ((k_ref.at[0], kall), (v_ref.at[0], vall), (gall.at[me], gall))
            )
        ]

    for d in range(1, sp):

        @pl.when(me + d < sp)
        def _(d=d):
            for copy in kv_copies(d, me):
                copy.start()

    for j in range(1, sp):

        @pl.when(j > me)
        def _(j=j):
            kall[j] = jnp.zeros(kall.shape[1:], BF16)
            vall[j] = jnp.zeros(vall.shape[1:], BF16)
            gall[j] = jnp.zeros(gall.shape[1:], F32)

    for h in range(heads):
        kv = h // repeat
        piece = (q_ref[0, :, h * HEAD_DIM : (h + 1) * HEAD_DIM].astype(F32) * HEAD_DIM**-0.5).astype(
            BF16
        )
        zero = jnp.zeros((rows, HEAD_DIM), BF16)
        parts = [piece if i == kv else zero for i in range(kv_heads)]
        qs[kv, (h % repeat) * rows : (h % repeat + 1) * rows, :] = jnp.concatenate(parts, axis=1)

    @pl.when(me > 0)
    def _():
        for copy in tail:
            copy.wait_recv()

    pad_ref[0:8, :] = jnp.where(me > 0, tails[...].astype(F32)[8:16], 0.0)
    filtered(16)
    conv_write = conv[:, width : width + STATE]
    turned_write = conv_write.astype(F32).T.astype(BF16)

    def st_copy(d, source, p):
        there = {"sp": lax.rem(me + d, sp)}
        ref = states.at[source, p] if p < pairs else decays.at[source]
        return remote(ref, ref, st_send.at[d, p], st_recv.at[source, p], there)

    for p in range(pairs):
        at = slice(p * LANES, (p + 1) * LANES)
        weighted = (conv[:, at].astype(F32) * end_wide[:, at]).astype(BF16)
        states[me, p] = jnp.dot(turned_write, weighted, preferred_element_type=F32).astype(BF16)
        for d in range(1, sp):

            @pl.when(me + d < sp)
            def _(d=d, p=p):
                if p == 0:
                    st_copy(d, me, pairs).start()
                st_copy(d, me, p).start()

    for j in range(sp - 1):

        @pl.when(j < me)
        def _(j=j):
            for copy in kv_copies(1, j):
                copy.wait_recv()

    keys = kall[...].reshape(sp * rows, -1)
    values = vall[...].reshape(sp * rows, -1)
    visible = [j * rows + col_id <= me * rows + row_id for j in range(sp)]
    for kv in range(kv_heads):
        own = lane // HEAD_DIM == kv
        summed_values = jnp.where(own, values, jnp.ones_like(values))
        scores = lax.dot_general(
            qs[kv], keys, (((1,), (1,)), ((), ())), preferred_element_type=F32
        )
        outs = []
        for i in range(repeat):
            h = kv * repeat + i
            gate_col = gate_cols[:, h : h + 1]
            tiles = [
                jnp.where(
                    visible[j],
                    scores[i * rows : (i + 1) * rows, j * rows : (j + 1) * rows]
                    + (gate_col - gall[j, h : h + 1, :]),
                    NEGATIVE,
                )
                for j in range(sp)
            ]
            top = tiles[0]
            for tile in tiles[1:]:
                top = jnp.maximum(top, tile)
            top = jnp.max(top, axis=1, keepdims=True)
            probs = jnp.concatenate([jnp.exp(tile - top).astype(BF16) for tile in tiles], axis=1)
            both = jnp.dot(probs, summed_values, preferred_element_type=F32)
            turned = pltpu.roll(both, HEAD_DIM, 1)
            outs.append(both / turned if h % 2 == kv else turned / both)
        for i in range(0, repeat, 2):
            h = kv * repeat + i
            acts[0, :, h * HEAD_DIM : (h + 2) * HEAD_DIM] = jnp.where(
                low, outs[i], outs[i + 1]
            ).astype(BF16)

    def act_copy(origin, hop):
        there = origin ^ hop
        return remote(
            acts.at[origin],
            acts.at[there],
            act_send.at[there],
            act_recv.at[there],
            {"fs": f ^ hop},
        )

    def piece_copy(p, origin, hop):
        there = origin ^ hop
        ref = pieces if p < pairs else scales
        index = (lambda slot: (p, slot)) if p < pairs else (lambda slot: (slot,))
        return remote(
            ref.at[index(origin)],
            ref.at[index(there)],
            piece_send.at[p, there],
            piece_recv.at[p, there],
            {"fs": f ^ hop},
        )

    act_copy(0, 1).start()
    act_copy(0, 2).start()

    exp_cum = jnp.exp(cum).T
    cum_col = cum.T
    conv_read = conv[:, width + STATE :]
    inner = lax.dot_general(
        conv_read, conv_write, (((1,), (1,)), ((), ())), preferred_element_type=F32
    )
    causal = row_id >= col_id
    for j in range(pairs):
        tile = conv[:, j * LANES : (j + 1) * LANES]
        parts = []
        for h in (2 * j, 2 * j + 1):
            gap = jnp.where(causal, cum_col[:, h : h + 1] - cum[h : h + 1, :], NEGATIVE)
            weights = (inner * (jnp.exp(gap) * step[h : h + 1, :])).astype(BF16)
            parts.append(jnp.dot(weights, tile, preferred_element_type=F32))
        bypass = jnp.where(low, bypass_ref[2 * j], bypass_ref[2 * j + 1])
        mix[:, j * LANES : (j + 1) * LANES] = (
            jnp.where(low, parts[0], parts[1]) + bypass * tile.astype(F32)
        )

    @pl.when(me > 0)
    def _():
        for j in range(sp - 1):

            @pl.when(j < me)
            def _(j=j):
                st_copy(1, j, pairs).wait_recv()

    squares = []

    def piece(p):
        at = slice(p * LANES, (p + 1) * LANES)
        carried[...] = jnp.zeros(carried.shape, F32)
        for j in range(sp - 1):

            @pl.when(j < me)
            def _(j=j):
                st_copy(1, j, p).wait_recv()
                decay = jnp.where(
                    low, decays[j, 2 * p : 2 * p + 1, :], decays[j, 2 * p + 1 : 2 * p + 2, :]
                )
                carried[...] = carried[...] * decay + states[j, p].astype(F32)

        entered = jnp.dot(conv_read, carried[...].astype(BF16), preferred_element_type=F32)
        gate = gate_ref[0, :, at].astype(F32)
        u = (mix[:, at] + entered * expand(exp_cum, p)) * (gate * jax.nn.sigmoid(gate))
        squares.append(u * u)
        pieces[p, 0] = (u * gain_ref[0:1, at]).astype(BF16)
        piece_copy(p, 0, 2).start()
        piece_copy(p, 0, 1).start()
        if p == pairs - 1:
            piece_copy(p, 0, 3).start()

    def pass_on(p):
        piece_copy(p, 0, 2).wait_recv()
        piece_copy(p, 2, 1).start()

    for p in range(pairs):
        piece(p)
        if p == pairs - 1:
            total = functools.reduce(jnp.add, squares)
            ones = jnp.ones((8, LANES), F32)
            mean = (
                lax.dot_general(
                    ones,
                    total,
                    (((1,), (1,)), ((), ())),
                    precision=lax.Precision.HIGHEST,
                    preferred_element_type=F32,
                )
                / width
            )
            scales[0] = lax.rsqrt(mean + EPSILON)
            for d in range(1, fs):
                piece_copy(pairs, 0, d).start()
        if p == min(1, pairs - 1):
            act_copy(0, 1).wait_recv()
            act_copy(1, 2).start()
        if p >= 1:
            pass_on(p - 1)

    def half_copy(d):
        return remote(
            half_out.at[d], half_in.at[d], half_send.at[d], half_recv.at[d], {"tp": 1 - t}
        )

    def give(d):
        there = pl.ds(pl.multiple_of((1 - t) * half, half), half)
        half_out[d] = acc[d, there, :].astype(BF16)
        half_copy(d).start()

    def sum_copy(d):
        return remote(sums.at[d], landed.at[d], sum_send.at[d], sum_recv.at[d], {"fs": f ^ d})

    def finish(d):
        half_copy(d).wait_recv()
        here = pl.ds(pl.multiple_of(t * half, half), half)
        total = (acc[d, here, :] + half_in[d].astype(F32)).astype(BF16)
        if d:
            sums[d] = total
            sum_copy(d).start()
        else:
            out_ref[0, :, pl.ds(pl.multiple_of(f * cols, cols), cols)] = total

    cut = (pairs - 1) * LANES

    def most(d):
        first = jnp.concatenate([pieces[p, d] for p in range(pairs - 1)], axis=1)
        acc[d] = jnp.dot(acts[d], wat_ref[...], preferred_element_type=F32)
        acc_state[d] = jnp.dot(first, wst_ref[0:cut, :], preferred_element_type=F32)

    def rest(d):
        last = jnp.dot(pieces[pairs - 1, d], wst_ref[cut:, :], preferred_element_type=F32)
        acc[d] += (acc_state[d] + last) * scales[d].T[:, 0:1]
        give(d)

    most(0)
    rest(0)
    act_copy(0, 2).wait_recv()
    most(2)
    act_copy(1, 2).wait_recv()
    for p in range(pairs - 1):
        piece_copy(p, 0, 1).wait_recv()
        piece_copy(p, 2, 1).wait_recv()
    most(1)
    most(3)
    for d in (2, 1, 3):
        piece_copy(pairs - 1, 0, d).wait_recv()
        piece_copy(pairs, 0, d).wait_recv()
        rest(d)
        if d == 2:
            finish(0)
    finish(2)
    finish(1)
    finish(3)
    for d in (2, 1, 3):
        sum_copy(d).wait_recv()
        out_ref[0, :, pl.ds(pl.multiple_of((f ^ d) * cols, cols), cols)] = landed[d]

    @pl.when(me < sp - 1)
    def _():
        for copy in tail:
            copy.wait_send()

    for d in range(1, sp):

        @pl.when(me + d < sp)
        def _(d=d):
            for copy in kv_copies(d, me) + [st_copy(d, me, p) for p in range(pairs + 1)]:
                copy.wait_send()

    for hop, origin in ((1, 0), (2, 0), (2, 1)):
        act_copy(origin, hop).wait_send()
    for p in range(pairs + 1):
        piece_copy(p, 0, 1).wait_send()
        piece_copy(p, 0, 2).wait_send()
        if p < pairs - 1:
            piece_copy(p, 2, 1).wait_send()
        else:
            piece_copy(p, 0, 3).wait_send()
    for d in range(fs):
        half_copy(d).wait_send()
    for d in range(1, fs):
        sum_copy(d).wait_send()


def fused(sp, fs, *args):
    x, w = args[0], args[1]
    rows, width = x.shape[1], x.shape[2]
    heads = args[4].shape[1]
    cols = args[16].shape[1]
    half = rows // 2
    args = list(args)
    args[11] = args[11].reshape(1, -1)
    args[15] = jnp.swapaxes(args[15], 1, 2)
    vmem = pl.BlockSpec(memory_space=pltpu.VMEM)
    smem = pl.BlockSpec(memory_space=pltpu.SMEM)
    specs = [smem if i in (6, 7) else vmem for i in range(len(args))]
    dma = pltpu.SemaphoreType.DMA
    kv_width = args[13].shape[2]
    kv_heads = kv_width // HEAD_DIM
    return pl.pallas_call(
        functools.partial(mixer_kernel, sp, fs),
        out_shape=jax.ShapeDtypeStruct((1, half, cols * fs), BF16),
        in_specs=specs,
        out_specs=vmem,
        scratch_shapes=[
            pltpu.VMEM((8 + rows, width + 2 * STATE), F32),
            pltpu.VMEM((16, width + 2 * STATE), BF16),
            pltpu.VMEM((rows, width + 2 * STATE), BF16),
            pltpu.VMEM((rows, width), F32),
            pltpu.VMEM((sp, rows, kv_width), BF16),
            pltpu.VMEM((sp, rows, kv_width), BF16),
            pltpu.VMEM((sp, heads, rows), F32),
            pltpu.VMEM((kv_heads, heads // kv_heads * rows, kv_width), BF16),
            pltpu.VMEM((sp, heads // 2, STATE, LANES), BF16),
            pltpu.VMEM((sp, heads, LANES), F32),
            pltpu.VMEM((STATE, LANES), F32),
            pltpu.VMEM((rows, width), F32),
            pltpu.VMEM((fs, rows, width), BF16),
            pltpu.VMEM((heads // 2, fs, rows, LANES), BF16),
            pltpu.VMEM((fs, 8, rows), F32),
            pltpu.VMEM((fs, rows, cols), F32),
            pltpu.VMEM((fs, rows, cols), F32),
            pltpu.VMEM((fs, half, cols), BF16),
            pltpu.VMEM((fs, half, cols), BF16),
            pltpu.VMEM((fs, half, cols), BF16),
            pltpu.VMEM((fs, half, cols), BF16),
            dma((3,)),
            dma((3,)),
            dma((sp, 3)),
            dma((sp, 3)),
            dma((sp, heads // 2 + 1)),
            dma((sp, heads // 2 + 1)),
            dma((fs,)),
            dma((fs,)),
            dma((heads // 2 + 1, fs)),
            dma((heads // 2 + 1, fs)),
            dma((fs,)),
            dma((fs,)),
            dma((fs,)),
            dma((fs,)),
        ],
        compiler_params=pltpu.CompilerParams(collective_id=0, has_side_effects=True),
    )(*args)


def one_kernel(*args, sp, fs, tp):
    rows, width = args[0].shape[1:]
    heads = args[4].shape[1]
    return (
        1 < sp <= 8
        and fs == 4
        and tp == 2
        and rows == LANES
        and args[1].shape[2] == STATE == LANES
        and width == heads * HEAD_DIM
        and args[12].shape[2] == width
        and args[13].shape[2] == 2 * HEAD_DIM
        and heads % 4 == 0
    )


def solution(mesh):
    in_specs = (
        P("fs", "sp", "tp"),
        P("fs", "sp", "tp"),
        P("fs", "sp", "tp"),
        P("fs", "sp", "tp"),
        P("fs", "tp", "sp"),
        P("fs", "tp", "sp"),
        P("tp"),
        P("tp"),
        P(None, "tp"),
        P(None, "tp"),
        P(None, "tp"),
        P("tp"),
        P("fs", "sp", "tp"),
        P("fs", "sp", "tp"),
        P("fs", "sp", "tp"),
        P("fs", "sp", "tp"),
        P("tp", "fs"),
        P("tp", "fs"),
    )
    out_specs = P("fs", ("sp", "tp"), None)
    sp, fs, tp = (mesh.shape[name] for name in ("sp", "fs", "tp"))

    def body(*args):
        if one_kernel(*args, sp=sp, fs=fs, tp=tp):
            return fused(sp, fs, *args)
        return shards(*args)

    return jax.shard_map(body, mesh=mesh, in_specs=in_specs, out_specs=out_specs, check_vma=False)
```

```python
import functools
import math

import jax
import jax.numpy as jnp
from jax import lax
from jax.experimental import pallas as pl
from jax.experimental.pallas import tpu as pltpu
from jax.sharding import PartitionSpec as P

HEAD_DIM = 64
STATE = 128


EPSILON = 1e-06
NEGATIVE = -1e30


def passed_along(shard, axis, by):
    devices = lax.axis_size(axis)
    pairs = [(i, i + by) for i in range(devices) if 0 <= i + by < devices]
    return lax.ppermute(shard, axis, pairs)


def entering(shard, axis, join, neutral):
    place = lax.axis_index(axis)
    gathered = jax.tree.map(
        lambda a, kind: lax.all_gather(a.astype(kind), axis), shard, (jnp.bfloat16, jnp.bfloat16)
    )
    state = jax.tree.map(lambda a, e: jnp.zeros_like(a) + jnp.asarray(e, a.dtype), shard, neutral)

    def one(hop, state):
        return join(
            state,
            jax.tree.map(
                lambda a, own: lax.dynamic_index_in_dim(a, hop, 0, False).astype(own.dtype),
                gathered,
                shard,
            ),
        )

    return lax.fori_loop(0, place, one, state)


def causal_filter(feeder_quantities, before, taps):
    length = feeder_quantities.shape[0]
    padded = jnp.concatenate([before, feeder_quantities], axis=0).astype(jnp.float32)
    summed = jnp.zeros(feeder_quantities.shape, jnp.float32)
    for offset in range(taps.shape[0]):
        summed = summed + taps[offset].astype(jnp.float32) * padded[offset : offset + length]
    return jax.nn.silu(summed).astype(jnp.bfloat16)


def compose(earlier, later):
    return (earlier[0] * later[0], earlier[1] * later[0][..., None, None] + later[1])


def shards(
    state_head_inputs,
    state_write_vectors,
    state_read_vectors,
    state_output_gate,
    presoftplus_steps,
    extra_decay_log,
    lane_shrinkage_powers,
    bypass_coefficient_vector,
    feeder_smoothing_stencil,
    stored_smoothing_stencil,
    lookup_smoothing_stencil,
    bundled_rescaling_vector,
    queries,
    attention_keys,
    attention_values,
    forget_gate_cumsum,
    state_out_weight,
    attention_out_weight,
):
    shard_rows = state_head_inputs.shape[1]
    input_rows = state_head_inputs[0]
    write_rows = state_write_vectors[0]
    read_rows = state_read_vectors[0]
    tap_rows = feeder_smoothing_stencil.shape[0] - 1
    value_width = input_rows.shape[1]
    vector_width = write_rows.shape[1]
    tail_rows = jnp.concatenate(
        [input_rows[-tap_rows:], write_rows[-tap_rows:], read_rows[-tap_rows:]], axis=1
    )
    before = passed_along(tail_rows, "sp", 1)
    conv_values = causal_filter(input_rows, before[:, :value_width], feeder_smoothing_stencil)
    conv_write = causal_filter(
        write_rows, before[:, value_width : value_width + vector_width], stored_smoothing_stencil
    )
    conv_read = causal_filter(
        read_rows, before[:, value_width + vector_width :], lookup_smoothing_stencil
    )
    stride_duration = jax.nn.softplus(presoftplus_steps[0])
    shrinkage_natural_power = (
        stride_duration * (-jnp.exp(lane_shrinkage_powers))[:, None] + extra_decay_log[0]
    )
    lane_tally = stride_duration.shape[0]
    groups = vector_width // STATE
    per_group = lane_tally // groups
    cumulative = jnp.cumsum(shrinkage_natural_power, axis=1)
    input_heads = conv_values.reshape(shard_rows, groups, per_group, HEAD_DIM)
    write_groups = conv_write.reshape(shard_rows, groups, STATE)
    read_groups = conv_read.reshape(shard_rows, groups, STATE)
    inner_products = jnp.einsum(
        "tgn,sgn->gts", read_groups, write_groups, preferred_element_type=jnp.float32
    )
    positions = jnp.arange(shard_rows)
    causal = positions[:, None] >= positions[None, :]
    log_gap = jnp.where(causal[None], cumulative[:, :, None] - cumulative[:, None, :], -jnp.inf)
    weights = jnp.exp(log_gap) * stride_duration[:, None, :]
    mix_weights = (
        inner_products[:, None] * weights.reshape(groups, per_group, shard_rows, shard_rows)
    ).astype(jnp.bfloat16)
    local_part = jnp.einsum(
        "ghts,sghp->tghp", mix_weights, input_heads, preferred_element_type=jnp.float32
    )
    end_scale = (jnp.exp(cumulative[:, -1:] - cumulative) * stride_duration).T.reshape(
        shard_rows, groups, per_group
    )
    weighted = (input_heads.astype(jnp.float32) * end_scale[..., None]).astype(jnp.bfloat16)
    block_state = jnp.einsum(
        "sghp,sgn->ghpn", weighted, write_groups, preferred_element_type=jnp.float32
    )
    total_decay = jnp.exp(cumulative[:, -1]).reshape(groups, per_group)
    identity = (jnp.ones_like(total_decay), jnp.zeros_like(block_state))
    carried = entering((total_decay, block_state), "sp", compose, identity)[1]
    carried_part = jnp.einsum(
        "tgn,ghpn->tghp",
        read_groups,
        carried.astype(jnp.bfloat16),
        preferred_element_type=jnp.float32,
    )
    carried_part = (
        carried_part * jnp.exp(cumulative).T.reshape(shard_rows, groups, per_group)[..., None]
    )
    mixer_sum = (
        local_part
        + carried_part
        + bypass_coefficient_vector.reshape(groups, per_group)[None, :, :, None]
        * input_heads.astype(jnp.float32)
    )
    gated_rows = mixer_sum.reshape(shard_rows, groups, per_group * HEAD_DIM) * jax.nn.silu(
        state_output_gate[0].astype(jnp.float32)
    ).reshape(shard_rows, groups, -1)
    stretch_coefficient = lax.rsqrt(
        jnp.mean(gated_rows * gated_rows, axis=-1, keepdims=True) + EPSILON
    )
    state_result = (
        (gated_rows * stretch_coefficient * bundled_rescaling_vector.reshape(groups, -1))
        .reshape(shard_rows, -1)
        .astype(jnp.bfloat16)
    )
    attend_heads = forget_gate_cumsum.shape[2]
    key_group_count = attention_keys.shape[2] // HEAD_DIM
    repeat_factor = attend_heads // key_group_count
    query_head_count = queries[0].reshape(shard_rows, key_group_count, repeat_factor, HEAD_DIM)
    first_query = lax.axis_index("sp") * shard_rows
    query_index = first_query + jnp.arange(shard_rows)
    last_query = first_query + shard_rows - 1
    query_gates = forget_gate_cumsum[0].T
    all_gates = lax.all_gather(forget_gate_cumsum[0], "sp", axis=0, tiled=True)
    attention_score_scale = HEAD_DIM ** (-0.5)
    starting = (
        jnp.full((attend_heads, shard_rows), NEGATIVE, jnp.float32),
        jnp.zeros((attend_heads, shard_rows), jnp.float32),
        jnp.zeros((attend_heads, shard_rows, HEAD_DIM), jnp.float32),
    )
    key_rows = lax.all_gather(attention_keys[0], "sp", axis=0, tiled=True)
    value_rows = lax.all_gather(attention_values[0], "sp", axis=0, tiled=True)
    span = key_rows.shape[0]
    sub_block = math.gcd(span, 512)

    def advance(sub_index, running):
        first_key = sub_index * sub_block

        def attend(running):
            running_max, running_sum, weighted_sum = running
            key_tile = lax.dynamic_slice_in_dim(
                key_rows, sub_index * sub_block, sub_block, 0
            ).reshape(sub_block, key_group_count, HEAD_DIM)
            value_tile = lax.dynamic_slice_in_dim(
                value_rows, sub_index * sub_block, sub_block, 0
            ).reshape(sub_block, key_group_count, HEAD_DIM)
            key_gates = lax.dynamic_slice_in_dim(all_gates, first_key, sub_block, 0)
            attention_scores = jnp.einsum(
                "ezxp,czp->zxec", query_head_count, key_tile, preferred_element_type=jnp.float32
            )
            attention_scores = (
                attention_scores.reshape(attend_heads, shard_rows, sub_block)
                * attention_score_scale
            )
            attention_scores = attention_scores + query_gates[:, :, None] - key_gates.T[:, None, :]
            visible = (first_key + jnp.arange(sub_block))[None, :] <= query_index[:, None]
            attention_scores = jnp.where(visible[None], attention_scores, NEGATIVE)
            new_max = jnp.maximum(running_max, jnp.max(attention_scores, axis=-1))
            shrink = jnp.exp(running_max - new_max)
            attention_probs = jnp.where(
                visible[None], jnp.exp(attention_scores - new_max[..., None]), 0.0
            )
            running_sum = running_sum * shrink + jnp.sum(attention_probs, axis=-1)
            weighted_value_sum = jnp.einsum(
                "fljx,xfc->fljc",
                attention_probs.astype(jnp.bfloat16).reshape(
                    key_group_count, repeat_factor, shard_rows, sub_block
                ),
                value_tile,
                preferred_element_type=jnp.float32,
            )
            weighted_sum = weighted_sum * shrink[..., None] + weighted_value_sum.reshape(
                attend_heads, shard_rows, HEAD_DIM
            )
            return (new_max, running_sum, weighted_sum)

        return lax.cond(first_key <= last_query, attend, lambda kept: kept, running)

    _, running_sum, weighted_sum = lax.fori_loop(0, span // sub_block, advance, starting)
    attend_out = (
        (weighted_sum / running_sum[..., None])
        .transpose(1, 0, 2)
        .reshape(shard_rows, -1)
        .astype(jnp.bfloat16)
    )
    state_columns, attend_columns = (
        lax.all_gather(state_out_weight, "fs", axis=1, tiled=True),
        lax.all_gather(attention_out_weight, "fs", axis=1, tiled=True),
    )
    summed = lax.psum_scatter(
        (
            jnp.dot(state_result, state_columns, preferred_element_type=jnp.float32)
            + jnp.dot(attend_out, attend_columns, preferred_element_type=jnp.float32)
        ).astype(jnp.bfloat16),
        "tp",
        scatter_dimension=0,
        tiled=True,
    )
    return summed[None]


MESH = pl.DeviceIdType.MESH
LANES = 128
BF16, F32 = jnp.bfloat16, jnp.float32


def mixer_kernel(
    sp,
    fs,
    x_ref,
    w_ref,
    r_ref,
    gate_ref,
    step_ref,
    extra_ref,
    shrink_ref,
    bypass_ref,
    tapx_ref,
    tapw_ref,
    tapr_ref,
    gain_ref,
    q_ref,
    k_ref,
    v_ref,
    forget_ref,
    wst_ref,
    wat_ref,
    out_ref,
    pad_ref,
    tails,
    conv,
    end_wide,
    kall,
    vall,
    gall,
    qs,
    own_state,
    state_in,
    state_out,
    mix,
    acts,
    pieces,
    scales,
    acc,
    acc_state,
    half_out,
    half_in,
    sums,
    landed,
    tail_send,
    tail_recv,
    kv_send,
    kv_recv,
    st_send,
    st_recv,
    act_send,
    act_recv,
    piece_send,
    piece_recv,
    half_send,
    half_recv,
    sum_send,
    sum_recv,
):
    me = lax.axis_index("sp")
    f = lax.axis_index("fs")
    t = lax.axis_index("tp")
    rows, width = x_ref.shape[1], x_ref.shape[2]
    heads = step_ref.shape[1]
    kv_heads = k_ref.shape[2] // HEAD_DIM
    repeat = heads // kv_heads
    pairs = heads // 2
    taps = tapx_ref.shape[0]
    cols = wst_ref.shape[1]
    half = rows // 2

    barrier = pltpu.get_barrier_semaphore()
    for d in range(1, sp):
        pl.semaphore_signal(
            barrier, inc=1, device_id={"sp": lax.rem(me + d, sp)}, device_id_type=MESH
        )
    for d in range(1, fs):
        pl.semaphore_signal(
            barrier, inc=1, device_id={"fs": lax.rem(f + d, fs)}, device_id_type=MESH
        )
    pl.semaphore_signal(barrier, inc=1, device_id={"tp": 1 - t}, device_id_type=MESH)

    def remote(src, dst, send, recv, where):
        return pltpu.make_async_remote_copy(
            src_ref=src,
            dst_ref=dst,
            send_sem=send,
            recv_sem=recv,
            device_id=where,
            device_id_type=MESH,
        )

    lane = lax.broadcasted_iota(jnp.int32, (1, LANES), 1)
    low = lane < HEAD_DIM
    row_id = lax.broadcasted_iota(jnp.int32, (rows, rows), 0)
    col_id = lax.broadcasted_iota(jnp.int32, (rows, rows), 1)

    def expand(columns, j):
        return jnp.where(low, columns[:, 2 * j : 2 * j + 1], columns[:, 2 * j + 1 : 2 * j + 2])

    gall[me] = forget_ref[0]
    gate_cols = forget_ref[0].T
    kall[me] = k_ref[0]
    vall[me] = v_ref[0]

    inputs = (
        (x_ref, tapx_ref, slice(0, width)),
        (w_ref, tapw_ref, slice(width, width + STATE)),
        (r_ref, tapr_ref, slice(width + STATE, width + 2 * STATE)),
    )

    def filtered(count):
        for _, tap_ref, at in inputs:
            total = jnp.zeros((count, at.stop - at.start), F32)
            for i in range(taps):
                first = 8 - (taps - 1) + i
                total = total + tap_ref[i : i + 1, :].astype(F32) * pad_ref[first : first + count, at]
            conv[0:count, at] = (total * jax.nn.sigmoid(total)).astype(BF16)

    pad_ref[0:8, :] = jnp.zeros((8, pad_ref.shape[1]), F32)
    for ref, _, at in inputs:
        pad_ref[8 : 8 + rows, at] = ref[0].astype(F32)
    filtered(rows)

    head_row = lax.broadcasted_iota(jnp.int32, (heads, rows), 0)
    power = jnp.zeros((heads, rows), F32)
    for h in range(heads):
        power = jnp.where(head_row == h, shrink_ref[h], power)
    presoft = step_ref[0]
    step = jnp.maximum(presoft, 0.0) + jnp.log1p(jnp.exp(-jnp.abs(presoft)))
    log_decay = extra_ref[0] - jnp.exp(power) * step
    upper = (row_id <= col_id).astype(F32)
    cum = jnp.dot(log_decay, upper, precision=lax.Precision.HIGHEST, preferred_element_type=F32)
    cum_end = cum[:, rows - 1 : rows]
    decays = jnp.broadcast_to(jnp.exp(cum_end), (heads, LANES))

    @pl.when(me == 0)
    def _():
        state_in[...] = jnp.zeros(state_in.shape, BF16)

    end_scale = (jnp.exp(cum_end - cum) * step).T
    for j in range(pairs):
        end_wide[:, j * LANES : (j + 1) * LANES] = expand(end_scale, j)

    pl.semaphore_wait(barrier, sp - 1 + fs - 1 + 1)

    tail = [
        remote(
            ref.at[0, rows - 16 : rows, :],
            tails.at[:, at],
            tail_send.at[i],
            tail_recv.at[i],
            {"sp": lax.rem(me + 1, sp)},
        )
        for i, (ref, _, at) in enumerate(inputs)
    ]

    @pl.when(me < sp - 1)
    def _():
        for copy in tail:
            copy.start()

    def kv_copies(d, source):
        there = {"sp": lax.rem(me + d, sp)}
        return [
            remote(src, dst.at[source], kv_send.at[d, i], kv_recv.at[source, i], there)
            for i, (src, dst) in enumerate(
                ((k_ref.at[0], kall), (v_ref.at[0], vall), (gall.at[me], gall))
            )
        ]

    for d in range(1, sp):

        @pl.when(me + d < sp)
        def _(d=d):
            for copy in kv_copies(d, me):
                copy.start()

    for j in range(1, sp):

        @pl.when(j > me)
        def _(j=j):
            kall[j] = jnp.zeros(kall.shape[1:], BF16)
            vall[j] = jnp.zeros(vall.shape[1:], BF16)
            gall[j] = jnp.zeros(gall.shape[1:], F32)

    for h in range(heads):
        kv = h // repeat
        piece = (q_ref[0, :, h * HEAD_DIM : (h + 1) * HEAD_DIM].astype(F32) * HEAD_DIM**-0.5).astype(
            BF16
        )
        zero = jnp.zeros((rows, HEAD_DIM), BF16)
        parts = [piece if i == kv else zero for i in range(kv_heads)]
        qs[kv, (h % repeat) * rows : (h % repeat + 1) * rows, :] = jnp.concatenate(parts, axis=1)

    @pl.when(me > 0)
    def _():
        for copy in tail:
            copy.wait_recv()

    pad_ref[0:8, :] = jnp.where(me > 0, tails[...].astype(F32)[8:16], 0.0)
    filtered(16)
    conv_write = conv[:, width : width + STATE]
    turned_write = conv_write.astype(F32).T.astype(BF16)

    def st_copy(p):
        there = {"sp": lax.rem(me + 1, sp)}
        return remote(state_out.at[p], state_in.at[p], st_send.at[p], st_recv.at[p], there)

    for p in range(pairs):
        at = slice(p * LANES, (p + 1) * LANES)
        weighted = (conv[:, at].astype(F32) * end_wide[:, at]).astype(BF16)
        own_state[p] = jnp.dot(turned_write, weighted, preferred_element_type=F32)

        @pl.when(me == 0)
        def _(p=p):
            state_out[p] = own_state[p].astype(BF16)
            st_copy(p).start()

    for j in range(sp - 1):

        @pl.when(j < me)
        def _(j=j):
            for copy in kv_copies(1, j):
                copy.wait_recv()

    keys = kall[...].reshape(sp * rows, -1)
    values = vall[...].reshape(sp * rows, -1)
    visible = [j * rows + col_id <= me * rows + row_id for j in range(sp)]
    for kv in range(kv_heads):
        own = lane // HEAD_DIM == kv
        summed_values = jnp.where(own, values, jnp.ones_like(values))
        scores = lax.dot_general(
            qs[kv], keys, (((1,), (1,)), ((), ())), preferred_element_type=F32
        )
        outs = []
        for i in range(repeat):
            h = kv * repeat + i
            gate_col = gate_cols[:, h : h + 1]
            tiles = [
                jnp.where(
                    visible[j],
                    scores[i * rows : (i + 1) * rows, j * rows : (j + 1) * rows]
                    + (gate_col - gall[j, h : h + 1, :]),
                    NEGATIVE,
                )
                for j in range(sp)
            ]
            top = tiles[0]
            for tile in tiles[1:]:
                top = jnp.maximum(top, tile)
            top = jnp.max(top, axis=1, keepdims=True)
            probs = jnp.concatenate([jnp.exp(tile - top).astype(BF16) for tile in tiles], axis=1)
            both = jnp.dot(probs, summed_values, preferred_element_type=F32)
            turned = pltpu.roll(both, HEAD_DIM, 1)
            outs.append(both / turned if h % 2 == kv else turned / both)
        for i in range(0, repeat, 2):
            h = kv * repeat + i
            acts[0, :, h * HEAD_DIM : (h + 2) * HEAD_DIM] = jnp.where(
                low, outs[i], outs[i + 1]
            ).astype(BF16)

    def act_copy(origin, hop):
        there = origin ^ hop
        return remote(
            acts.at[origin],
            acts.at[there],
            act_send.at[there],
            act_recv.at[there],
            {"fs": f ^ hop},
        )

    def piece_copy(p, origin, hop):
        there = origin ^ hop
        ref = pieces if p < pairs else scales
        index = (lambda slot: (p, slot)) if p < pairs else (lambda slot: (slot,))
        return remote(
            ref.at[index(origin)],
            ref.at[index(there)],
            piece_send.at[p, there],
            piece_recv.at[p, there],
            {"fs": f ^ hop},
        )

    act_copy(0, 1).start()
    act_copy(0, 2).start()

    @pl.when(jnp.logical_and(me > 0, me < sp - 1))
    def _():
        for p in range(pairs):
            st_copy(p).wait_recv()
            decay = jnp.where(low, decays[2 * p : 2 * p + 1, :], decays[2 * p + 1 : 2 * p + 2, :])
            state_out[p] = (state_in[p].astype(F32) * decay + own_state[p]).astype(BF16)
            st_copy(p).start()

    exp_cum = jnp.exp(cum).T
    cum_col = cum.T
    conv_read = conv[:, width + STATE :]
    inner = lax.dot_general(
        conv_read, conv_write, (((1,), (1,)), ((), ())), preferred_element_type=F32
    )
    causal = row_id >= col_id
    for j in range(pairs):
        tile = conv[:, j * LANES : (j + 1) * LANES]
        parts = []
        for h in (2 * j, 2 * j + 1):
            gap = jnp.where(causal, cum_col[:, h : h + 1] - cum[h : h + 1, :], NEGATIVE)
            weights = (inner * (jnp.exp(gap) * step[h : h + 1, :])).astype(BF16)
            parts.append(jnp.dot(weights, tile, preferred_element_type=F32))
        bypass = jnp.where(low, bypass_ref[2 * j], bypass_ref[2 * j + 1])
        mix[:, j * LANES : (j + 1) * LANES] = (
            jnp.where(low, parts[0], parts[1]) + bypass * tile.astype(F32)
        )

    squares = []

    def piece(p):
        at = slice(p * LANES, (p + 1) * LANES)

        @pl.when(me == sp - 1)
        def _():
            st_copy(p).wait_recv()

        entered = jnp.dot(conv_read, state_in[p], preferred_element_type=F32)
        gate = gate_ref[0, :, at].astype(F32)
        u = (mix[:, at] + entered * expand(exp_cum, p)) * (gate * jax.nn.sigmoid(gate))
        squares.append(u * u)
        pieces[p, 0] = (u * gain_ref[0:1, at]).astype(BF16)
        piece_copy(p, 0, 2).start()
        piece_copy(p, 0, 1).start()
        if p == pairs - 1:
            piece_copy(p, 0, 3).start()

    def pass_on(p):
        piece_copy(p, 0, 2).wait_recv()
        piece_copy(p, 2, 1).start()

    for p in range(pairs):
        piece(p)
        if p == pairs - 1:
            total = functools.reduce(jnp.add, squares)
            ones = jnp.ones((8, LANES), F32)
            mean = (
                lax.dot_general(
                    ones,
                    total,
                    (((1,), (1,)), ((), ())),
                    precision=lax.Precision.HIGHEST,
                    preferred_element_type=F32,
                )
                / width
            )
            scales[0] = lax.rsqrt(mean + EPSILON)
            for d in range(1, fs):
                piece_copy(pairs, 0, d).start()
        if p == min(1, pairs - 1):
            act_copy(0, 1).wait_recv()
            act_copy(1, 2).start()
        if p >= 1:
            pass_on(p - 1)

    def half_copy(d):
        return remote(
            half_out.at[d], half_in.at[d], half_send.at[d], half_recv.at[d], {"tp": 1 - t}
        )

    def give(d):
        there = pl.ds(pl.multiple_of((1 - t) * half, half), half)
        half_out[d] = acc[d, there, :].astype(BF16)
        half_copy(d).start()

    def sum_copy(d):
        return remote(sums.at[d], landed.at[d], sum_send.at[d], sum_recv.at[d], {"fs": f ^ d})

    def finish(d):
        half_copy(d).wait_recv()
        here = pl.ds(pl.multiple_of(t * half, half), half)
        total = (acc[d, here, :] + half_in[d].astype(F32)).astype(BF16)
        if d:
            sums[d] = total
            sum_copy(d).start()
        else:
            out_ref[0, :, pl.ds(pl.multiple_of(f * cols, cols), cols)] = total

    cut = (pairs - 1) * LANES

    def most(d):
        first = jnp.concatenate([pieces[p, d] for p in range(pairs - 1)], axis=1)
        acc[d] = jnp.dot(acts[d], wat_ref[...], preferred_element_type=F32)
        acc_state[d] = jnp.dot(first, wst_ref[0:cut, :], preferred_element_type=F32)

    def rest(d):
        last = jnp.dot(pieces[pairs - 1, d], wst_ref[cut:, :], preferred_element_type=F32)
        acc[d] += (acc_state[d] + last) * scales[d].T[:, 0:1]
        give(d)

    most(0)
    rest(0)
    act_copy(0, 2).wait_recv()
    most(2)
    act_copy(1, 2).wait_recv()
    for p in range(pairs - 1):
        piece_copy(p, 0, 1).wait_recv()
        piece_copy(p, 2, 1).wait_recv()
    most(1)
    most(3)
    for d in (2, 1, 3):
        piece_copy(pairs - 1, 0, d).wait_recv()
        piece_copy(pairs, 0, d).wait_recv()
        rest(d)
        if d == 2:
            finish(0)
    finish(2)
    finish(1)
    finish(3)
    for d in (2, 1, 3):
        sum_copy(d).wait_recv()
        out_ref[0, :, pl.ds(pl.multiple_of((f ^ d) * cols, cols), cols)] = landed[d]

    @pl.when(me < sp - 1)
    def _():
        for copy in tail + [st_copy(p) for p in range(pairs)]:
            copy.wait_send()

    for d in range(1, sp):

        @pl.when(me + d < sp)
        def _(d=d):
            for copy in kv_copies(d, me):
                copy.wait_send()

    for hop, origin in ((1, 0), (2, 0), (2, 1)):
        act_copy(origin, hop).wait_send()
    for p in range(pairs + 1):
        piece_copy(p, 0, 1).wait_send()
        piece_copy(p, 0, 2).wait_send()
        if p < pairs - 1:
            piece_copy(p, 2, 1).wait_send()
        else:
            piece_copy(p, 0, 3).wait_send()
    for d in range(fs):
        half_copy(d).wait_send()
    for d in range(1, fs):
        sum_copy(d).wait_send()


def fused(sp, fs, *args):
    x, w = args[0], args[1]
    rows, width = x.shape[1], x.shape[2]
    heads = args[4].shape[1]
    cols = args[16].shape[1]
    half = rows // 2
    args = list(args)
    args[11] = args[11].reshape(1, -1)
    args[15] = jnp.swapaxes(args[15], 1, 2)
    vmem = pl.BlockSpec(memory_space=pltpu.VMEM)
    smem = pl.BlockSpec(memory_space=pltpu.SMEM)
    specs = [smem if i in (6, 7) else vmem for i in range(len(args))]
    dma = pltpu.SemaphoreType.DMA
    kv_width = args[13].shape[2]
    kv_heads = kv_width // HEAD_DIM
    return pl.pallas_call(
        functools.partial(mixer_kernel, sp, fs),
        out_shape=jax.ShapeDtypeStruct((1, half, cols * fs), BF16),
        in_specs=specs,
        out_specs=vmem,
        scratch_shapes=[
            pltpu.VMEM((8 + rows, width + 2 * STATE), F32),
            pltpu.VMEM((16, width + 2 * STATE), BF16),
            pltpu.VMEM((rows, width + 2 * STATE), BF16),
            pltpu.VMEM((rows, width), F32),
            pltpu.VMEM((sp, rows, kv_width), BF16),
            pltpu.VMEM((sp, rows, kv_width), BF16),
            pltpu.VMEM((sp, heads, rows), F32),
            pltpu.VMEM((kv_heads, heads // kv_heads * rows, kv_width), BF16),
            pltpu.VMEM((heads // 2, STATE, LANES), F32),
            pltpu.VMEM((heads // 2, STATE, LANES), BF16),
            pltpu.VMEM((heads // 2, STATE, LANES), BF16),
            pltpu.VMEM((rows, width), F32),
            pltpu.VMEM((fs, rows, width), BF16),
            pltpu.VMEM((heads // 2, fs, rows, LANES), BF16),
            pltpu.VMEM((fs, 8, rows), F32),
            pltpu.VMEM((fs, rows, cols), F32),
            pltpu.VMEM((fs, rows, cols), F32),
            pltpu.VMEM((fs, half, cols), BF16),
            pltpu.VMEM((fs, half, cols), BF16),
            pltpu.VMEM((fs, half, cols), BF16),
            pltpu.VMEM((fs, half, cols), BF16),
            dma((3,)),
            dma((3,)),
            dma((sp, 3)),
            dma((sp, 3)),
            dma((heads // 2,)),
            dma((heads // 2,)),
            dma((fs,)),
            dma((fs,)),
            dma((heads // 2 + 1, fs)),
            dma((heads // 2 + 1, fs)),
            dma((fs,)),
            dma((fs,)),
            dma((fs,)),
            dma((fs,)),
        ],
        compiler_params=pltpu.CompilerParams(collective_id=0, has_side_effects=True),
    )(*args)


def one_kernel(*args, sp, fs, tp):
    rows, width = args[0].shape[1:]
    heads = args[4].shape[1]
    return (
        1 < sp <= 8
        and fs == 4
        and tp == 2
        and rows == LANES
        and args[1].shape[2] == STATE == LANES
        and width == heads * HEAD_DIM
        and args[12].shape[2] == width
        and args[13].shape[2] == 2 * HEAD_DIM
        and heads % 4 == 0
    )


def solution(mesh):
    in_specs = (
        P("fs", "sp", "tp"),
        P("fs", "sp", "tp"),
        P("fs", "sp", "tp"),
        P("fs", "sp", "tp"),
        P("fs", "tp", "sp"),
        P("fs", "tp", "sp"),
        P("tp"),
        P("tp"),
        P(None, "tp"),
        P(None, "tp"),
        P(None, "tp"),
        P("tp"),
        P("fs", "sp", "tp"),
        P("fs", "sp", "tp"),
        P("fs", "sp", "tp"),
        P("fs", "sp", "tp"),
        P("tp", "fs"),
        P("tp", "fs"),
    )
    out_specs = P("fs", ("sp", "tp"), None)
    sp, fs, tp = (mesh.shape[name] for name in ("sp", "fs", "tp"))

    def body(*args):
        if one_kernel(*args, sp=sp, fs=fs, tp=tp):
            return fused(sp, fs, *args)
        return shards(*args)

    return jax.shard_map(body, mesh=mesh, in_specs=in_specs, out_specs=out_specs, check_vma=False)
```
